256 devices in a mesh: sp: 64 (over z, y, core), tp: 4 (over x).
Axes of the slice: x: 4, y: 4, z: 8, core: 2. Of those that a mesh axis runs over, the one named last changes fastest.
Arguments:
- tokens: bfloat16 [16384, 4096], P(('sp', 'tp')), may hold values from -6 to 6
- norm_gain: float32 [4096], replicated, may hold values from 0.1 to 1.9
- w_query: bfloat16 [4096, 1024], P(None, 'tp'), may hold values from -0.25 to 0.25
- w_key: bfloat16 [4096, 512], P(None, 'tp'), may hold values from -0.09375 to 0.09375
- w_value: bfloat16 [4096, 512], P(None, 'tp'), may hold values from -0.09375 to 0.09375
- score_shift: float32 [8], P('tp'), may hold values from -15 to -8
- w_conv_b: bfloat16 [4096, 1024], P(None, 'tp'), may hold values from -0.09375 to 0.09375
- w_conv_c: bfloat16 [4096, 1024], P(None, 'tp'), may hold values from -0.09375 to 0.09375
- w_conv_u: bfloat16 [4096, 1024], P(None, 'tp'), may hold values from -0.09375 to 0.09375
- conv_kernel: float32 [3, 1024], P(None, 'tp'), may hold values from -3.5 to 3.5
- w_out_att: bfloat16 [4096, 1024], P('sp', 'tp'), may hold values from -0.75 to 0.75
- w_out_conv: bfloat16 [4096, 1024], P('sp', 'tp'), may hold values from -0.1875 to 0.1875
Outputs:
- mixed: bfloat16 [16384, 4096], P(('sp', 'tp'))
- log_weight: float32 [16384, 8], P('sp', 'tp')
The draws below stay inside these ranges and needn't reach their ends.
All inputs are finite; a program needn't handle non-finite values.
Results may differ from the reference program's by a relative error of at most 0.017.
Values may be sent and summed in bfloat16 or wider, within the bound.
A program may use at most 128 MiB of HBM per device.

```python
import jax
import jax.numpy as jnp
from jax import lax

D = 4096
ATT_HEADS = 8
KV_HEADS = 4
HEAD_DIM = 128
CONV_W = 1024
CONV_K = 3
KEY_BLOCK = 1024
TOK_DEV = 256
ATT_W = 1024
TOKENS = 16384
N_TP = 4


def draw_score_shift(key, part):
    return jax.random.uniform(key, (ATT_HEADS,), jnp.float32, -13.0, -8.0)


def levels(rng, extent, shards, low, high):
    factor_of, own = 1.0, jax.random.fold_in(rng, 6)
    for position, blocks in shards:
        heights = jnp.exp(jax.random.uniform(jax.random.fold_in(own, position), (blocks,), jnp.float32, low / len(shards), high / len(shards)))
        factor_of = factor_of * jnp.repeat(heights, extent[position] // blocks).reshape([-1 if axis == position else 1 for axis in range(len(extent))])
    return factor_of


def bell_draw(key, extent, spread, most, split=(), kind=jnp.bfloat16):
    gain = levels(key, extent, split, -0.22, 0.18) if split else 1.0
    entries = jax.random.normal(key, extent, jnp.float32) * spread * gain
    return jnp.minimum(jnp.maximum(entries, -most), most).astype(kind)


def setup_inputs(seed: int = 0) -> dict:
    splits = jax.random.split(jax.random.key(seed), 13)
    tokens = bell_draw(splits[0], (TOKENS, D), 1.0, 6.0, ((0, 256),))
    norm_gain = jnp.clip(1.0 + 0.18 * jax.random.normal(splits[1], (D,), jnp.float32), 0.1, 1.9)
    w_query = bell_draw(splits[2], (D, ATT_W), (D // 9) ** -0.5, 0.25, ((1, 4),))
    w_key = bell_draw(splits[3], (D, KV_HEADS * HEAD_DIM), D ** -0.5, 0.09375, ((1, 4),))
    w_value = bell_draw(splits[4], (D, KV_HEADS * HEAD_DIM), D ** -0.5, 0.09375, ((1, 4),))
    score_shift = draw_score_shift(jax.random.fold_in(splits[12], 71), 0)
    w_conv_b = bell_draw(splits[6], (D, CONV_W), D ** -0.5, 0.09375, ((1, 4),))
    w_conv_c = bell_draw(splits[7], (D, CONV_W), D ** -0.5, 0.09375, ((1, 4),))
    w_conv_u = bell_draw(splits[8], (D, CONV_W), D ** -0.5, 0.09375, ((1, 4),))
    conv_kernel = bell_draw(splits[9], (CONV_K, CONV_W), CONV_K ** -0.5, 3.5, ((1, 4),), jnp.float32)
    w_out_att = bell_draw(splits[10], (D, ATT_W), (ATT_W // 16) ** -0.5, 0.75, ((0, 64), (1, 4)))
    w_out_conv = bell_draw(splits[11], (D, CONV_W), CONV_W ** -0.5, 0.1875, ((0, 64), (1, 4)))
    return {"tokens": tokens, "norm_gain": norm_gain, "w_query": w_query, "w_key": w_key, "w_value": w_value, "score_shift": score_shift, "w_conv_b": w_conv_b, "w_conv_c": w_conv_c, "w_conv_u": w_conv_u, "conv_kernel": conv_kernel, "w_out_att": w_out_att, "w_out_conv": w_out_conv}


def normalize(tokens, norm_gain):
    widened = tokens.astype(jnp.float32)
    inverse = lax.rsqrt(lax.optimization_barrier(jnp.mean(widened * widened, axis=-1, keepdims=True)) + 1e-06)
    return (widened * inverse * norm_gain).astype(jnp.bfloat16)

def block_terms(grouped_q, key_block, value_block, shifts, query_pos, key_first):
    scores = jnp.einsum('qhgd,khd->qhgk', grouped_q.astype(jnp.float32), key_block.astype(jnp.float32))
    scores = scores * HEAD_DIM ** (-0.5) + shifts[None, :, :, None]
    key_pos = key_first + jnp.arange(KEY_BLOCK, dtype=jnp.int32)
    causal = key_pos[None, None, None, :] < query_pos[:, None, None, None]
    soft = jnp.where(causal, jax.nn.softplus(scores), 0.0)
    after_sum = lax.cumsum(soft, axis=3, reverse=True) - soft
    relative = jnp.where(causal, jnp.exp(jax.nn.log_sigmoid(scores) - after_sum), 0.0).astype(jnp.bfloat16)
    partial_value = jnp.einsum('qhgk,khd->qhgd', relative.astype(jnp.float32), value_block.astype(jnp.float32))
    return (partial_value, lax.optimization_barrier(jnp.sum(soft, axis=3)))

def reference(tokens, norm_gain, w_query, w_key, w_value, score_shift, w_conv_b, w_conv_c, w_conv_u, conv_kernel, w_out_att, w_out_conv):
    normed = normalize(tokens, norm_gain)

    def project(weight):
        return jnp.dot(normed, weight, preferred_element_type=jnp.float32).astype(jnp.bfloat16)
    queries = project(w_query)
    keys = project(w_key)
    values = project(w_value)
    gate_b = project(w_conv_b)
    gate_c = project(w_conv_c)
    inputs_u = project(w_conv_u)
    grouping = ATT_HEADS // KV_HEADS
    shifts = score_shift.reshape(KV_HEADS, grouping)
    key_blocks = keys.reshape(TOKENS // KEY_BLOCK, KEY_BLOCK, KV_HEADS, HEAD_DIM)
    value_blocks = values.reshape(TOKENS // KEY_BLOCK, KEY_BLOCK, KV_HEADS, HEAD_DIM)
    key_firsts = jnp.arange(TOKENS // KEY_BLOCK, dtype=jnp.int32) * KEY_BLOCK
    query_blocks = queries.reshape(TOKENS // TOK_DEV, TOK_DEV, KV_HEADS, grouping, HEAD_DIM)
    query_firsts = jnp.arange(TOKENS // TOK_DEV, dtype=jnp.int32) * TOK_DEV

    def per_query(inputs):
        grouped_q, query_first = inputs
        query_pos = query_first + jnp.arange(TOK_DEV, dtype=jnp.int32)

        def per_key(key_inputs):
            key_block, value_block, key_first = key_inputs
            return block_terms(grouped_q, key_block, value_block, shifts, query_pos, key_first)
        partials, totals = lax.map(per_key, (key_blocks, value_blocks, key_firsts))
        later_sum = lax.cumsum(totals, axis=0, reverse=True) - totals
        attended = lax.optimization_barrier(jnp.sum(jnp.exp(-later_sum)[..., None] * partials, axis=0))
        sums_all = lax.optimization_barrier(jnp.sum(totals, axis=0))
        return (attended.reshape(TOK_DEV, ATT_W), sums_all.reshape(TOK_DEV, ATT_HEADS))
    attended, sums_all = lax.map(per_query, (query_blocks, query_firsts))
    attended = attended.reshape(TOKENS, ATT_W).astype(jnp.bfloat16)
    log_weight = jnp.log(jnp.maximum(-jnp.expm1(-sums_all.reshape(TOKENS, ATT_HEADS)), 0.05))
    products = (gate_c.astype(jnp.float32) * inputs_u.astype(jnp.float32)).astype(jnp.bfloat16)
    padded = jnp.concatenate([jnp.zeros((CONV_K - 1, CONV_W), jnp.bfloat16), products], axis=0)
    summed = jnp.zeros((TOKENS, CONV_W), jnp.float32)
    for tap in range(CONV_K):
        summed = summed + conv_kernel[tap][None, :] * padded[tap:tap + TOKENS].astype(jnp.float32)
    convolved = (gate_b.astype(jnp.float32) * summed).astype(jnp.bfloat16)
    att_cols = ATT_W // N_TP
    conv_cols = CONV_W // N_TP
    contract = (((1,), (1,)), ((), ()))
    mixed_sum = jnp.zeros((TOKENS, D), jnp.float32)
    for shard_no in range(N_TP):
        att_part = attended[:, shard_no * att_cols:(shard_no + 1) * att_cols]
        att_rows = w_out_att[:, shard_no * att_cols:(shard_no + 1) * att_cols]
        conv_part = convolved[:, shard_no * conv_cols:(shard_no + 1) * conv_cols]
        conv_rows = w_out_conv[:, shard_no * conv_cols:(shard_no + 1) * conv_cols]
        share = lax.dot_general(att_part, att_rows, contract, preferred_element_type=jnp.float32)
        share = share + lax.dot_general(conv_part, conv_rows, contract, preferred_element_type=jnp.float32)
        mixed_sum = mixed_sum + share.astype(jnp.bfloat16).astype(jnp.float32)
    return (mixed_sum.astype(jnp.bfloat16), log_weight)
```

```python
import jax
import jax.numpy as jnp
from jax import lax
from jax.experimental import pallas as pl
from jax.experimental.pallas import tpu as pltpu
from jax.sharding import PartitionSpec as P

HEAD_DIM = 128
CONV_K = 3


def laid_out(blocks, dim):
    blocks = jnp.moveaxis(blocks, 0, dim)
    lengths = blocks.shape
    return blocks.reshape(*lengths[:dim], lengths[dim] * lengths[dim + 1], *lengths[dim + 2 :])


def copy_for_each(x, axis):
    count = lax.axis_size(axis)
    return lax.all_to_all(jnp.broadcast_to(x[None], (count, *x.shape)), axis, 0, 0, tiled=True)


def gathered_copies(x, axis, dim):
    return laid_out(copy_for_each(x, axis), dim)


def shifted(value, axis, steps):
    count = lax.axis_size(axis)
    leading, last = (max(0, -steps), min(count, count - steps))
    return lax.ppermute(value, axis, [(source, source + steps) for source in range(leading, last)])


def sent_together(arrays, axis, dim, along):
    both = jnp.concatenate(arrays, axis=along)
    out, at, finished = (lax.all_gather(both, axis, axis=dim, tiled=True), 0, [])
    for a in arrays:
        finished.append(lax.slice_in_dim(out, at, at + a.shape[along], axis=along))
        at += a.shape[along]
    return tuple(finished)


def normalize(tokens, norm_gain):
    widened = tokens.astype(jnp.float32)
    inverse = lax.rsqrt(jnp.mean(widened * widened, axis=-1, keepdims=True) + 1e-06)
    return (widened * inverse * norm_gain).astype(jnp.bfloat16)


F32 = jnp.float32
BF16 = jnp.bfloat16
TILE = 256
NT = (((1,), (1,)), ((), ()))


def softplus(z):
    small = jnp.exp(-jnp.abs(z))
    whole = 1.0 + small
    return jnp.maximum(z, 0.0) + (jnp.log(whole) + (small - (whole - 1.0)))


def attention_kernel(
    q_ref, k_ref, v_ref, shift_ref, later_ref, out_ref, sum_ref, q_split, acc, carry, score, base, after
):
    last = lax.axis_index("sp")
    heads = [pl.ds(0, TILE), pl.ds(TILE, TILE)]
    for h in range(2):
        scaled = q_ref[:, h * HEAD_DIM : (h + 1) * HEAD_DIM].astype(F32) * HEAD_DIM ** (-0.5)
        high = scaled.astype(BF16)
        q_split[heads[h], 0:HEAD_DIM] = high
        q_split[heads[h], HEAD_DIM : 2 * HEAD_DIM] = (scaled - high.astype(F32)).astype(BF16)
    acc[...] = jnp.zeros_like(acc)
    carry[...] = jnp.zeros_like(carry)

    def rows_of(tile):
        return pl.ds(pl.multiple_of(jnp.maximum(tile, 0) * TILE, TILE), TILE)

    def scores(tile, slot):
        key = k_ref[rows_of(tile), :]
        twice = jnp.concatenate([key, key], axis=1)
        for h in range(2):
            score[slot, heads[h], :] = (
                lax.dot_general(q_split[heads[h], :], twice, NT, preferred_element_type=F32)
                + shift_ref[h]
            )

    def sums(slot, masked=False):
        for h in range(2):
            z = score[slot, heads[h], :]
            soft = softplus(z)
            if masked:
                row = lax.broadcasted_iota(jnp.int32, (TILE, TILE), 0)
                col = lax.broadcasted_iota(jnp.int32, (TILE, TILE), 1)
                soft = jnp.where(col < row, soft, 0.0)
                z = jnp.where(col < row, z, -jnp.inf)
            held = carry[heads[h], :]
            base[slot, heads[h], :] = (z - soft) - jnp.concatenate([held, held], axis=1)
            after[slot, heads[h], :] = jnp.dot(
                soft.astype(BF16), later_ref[...], preferred_element_type=F32
            )
            carry[heads[h], :] = held + jnp.sum(soft, axis=1, keepdims=True)

    def weigh(tile, slot):
        value = v_ref[rows_of(tile), :]
        for h in range(2):
            weight = jnp.exp(base[slot, heads[h], :] - after[slot, heads[h], :])
            acc[heads[h], :] += jnp.dot(weight.astype(BF16), value, preferred_element_type=F32)

    scores(last, 0)
    sums(0, True)
    scores(last - 1, 1)

    def two_tiles(step, _):
        tile = last - 1 - 2 * step
        scores(tile - 1, 0)
        sums(1)
        weigh(tile + 1, 0)
        scores(tile - 2, 1)
        sums(0)
        weigh(tile, 1)
        return 0

    lax.fori_loop(0, last // 2, two_tiles, 0)

    @pl.when(last % 2 == 1)
    def _():
        sums(1)
        weigh(1, 0)
        weigh(0, 1)

    @pl.when(last % 2 == 0)
    def _():
        weigh(0, 0)

    for h in range(2):
        out_ref[:, h * HEAD_DIM : (h + 1) * HEAD_DIM] = acc[heads[h], :].astype(BF16)
        sum_ref[:, h * HEAD_DIM : (h + 1) * HEAD_DIM] = carry[heads[h], :]


def attend(queries, key_whole, value_whole, score_shift):
    row_count, width = queries.shape
    later = (jnp.arange(TILE)[:, None] > jnp.arange(TILE)[None, :]).astype(BF16)
    vmem = pl.BlockSpec(memory_space=pltpu.VMEM)
    attended, sums = pl.pallas_call(
        attention_kernel,
        name="attention",
        out_shape=(
            jax.ShapeDtypeStruct((row_count, width), BF16),
            jax.ShapeDtypeStruct((row_count, width), F32),
        ),
        in_specs=[vmem, vmem, vmem, pl.BlockSpec(memory_space=pltpu.SMEM), vmem],
        out_specs=(vmem, vmem),
        scratch_shapes=[
            pltpu.VMEM((2 * TILE, 2 * HEAD_DIM), BF16),
            pltpu.VMEM((2 * TILE, HEAD_DIM), F32),
            pltpu.VMEM((2 * TILE, HEAD_DIM), F32),
            pltpu.VMEM((2, 2 * TILE, TILE), F32),
            pltpu.VMEM((2, 2 * TILE, TILE), F32),
            pltpu.VMEM((2, 2 * TILE, TILE), F32),
        ],
        compiler_params=pltpu.CompilerParams(vmem_limit_bytes=40 * 1024 * 1024),
        cost_estimate=pl.CostEstimate(
            flops=12 * 10**9, bytes_accessed=9 * 10**6, transcendentals=25 * 10**6
        ),
    )(queries, key_whole, value_whole, score_shift, later)
    return attended, sums[:, ::HEAD_DIM]


def local(
    tokens,
    norm_gain,
    w_query,
    w_key,
    w_value,
    score_shift,
    w_conv_b,
    w_conv_c,
    w_conv_u,
    conv_kernel,
    w_out_att,
    w_out_conv,
):
    weights = (w_query, w_key, w_value, w_conv_b, w_conv_c, w_conv_u)

    def project(rows_in):
        normed = normalize(rows_in, norm_gain)
        return jnp.concatenate(
            [
                jnp.dot(normed, weight, preferred_element_type=jnp.float32).astype(jnp.bfloat16)
                for weight in weights
            ],
            axis=1,
        )

    projected = project(gathered_copies(tokens, "tp", 0))
    widths = [weight.shape[1] for weight in weights]
    edges = [0]
    for width in widths:
        edges.append(edges[-1] + width)
    queries, keys, values, gate_b, gate_c, inputs_u = [
        projected[:, edges[pos] : edges[pos + 1]] for pos in range(6)
    ]
    tok_count = projected.shape[0]
    conv_local = gate_b.shape[1]
    products = (gate_c.astype(jnp.float32) * inputs_u.astype(jnp.float32)).astype(jnp.bfloat16)
    previous = shifted(products[tok_count - (CONV_K - 1) :], "sp", 1)
    key_whole, value_whole, att_rows, conv_rows = (
        *sent_together((keys, values), "sp", 0, 1),
        *sent_together((w_out_att, w_out_conv), "sp", 0, 1),
    )
    attended, sums_all = attend(queries, key_whole, value_whole, score_shift)
    log_weight = jnp.log(jnp.maximum(-jnp.expm1(-sums_all), 0.05))
    extended = jnp.concatenate([previous, products], axis=0)
    summed = jnp.zeros((tok_count, conv_local), jnp.float32)
    for tap in range(CONV_K):
        summed = summed + conv_kernel[tap][None, :] * extended[tap : tap + tok_count].astype(
            jnp.float32
        )
    convolved = (gate_b.astype(jnp.float32) * summed).astype(jnp.bfloat16)
    contract = (((1,), (1,)), ((), ()))
    share = lax.dot_general(attended, att_rows, contract, preferred_element_type=jnp.float32)
    share = share + lax.dot_general(
        convolved, conv_rows, contract, preferred_element_type=jnp.float32
    )
    rounded = share.astype(jnp.bfloat16).astype(jnp.float32)
    mixed = lax.psum_scatter(rounded.astype(jnp.bfloat16), "tp", scatter_dimension=0, tiled=True)
    return (mixed, log_weight)


def solution(mesh):
    return jax.shard_map(
        local,
        mesh=mesh,
        in_specs=(
            P(("sp", "tp"), None),
            P(),
            P(None, "tp"),
            P(None, "tp"),
            P(None, "tp"),
            P("tp"),
            P(None, "tp"),
            P(None, "tp"),
            P(None, "tp"),
            P(None, "tp"),
            P("sp", "tp"),
            P("sp", "tp"),
        ),
        out_specs=(P(("sp", "tp"), None), P("sp", "tp")),
        check_vma=False,
    )
```

```python
import jax
import jax.numpy as jnp
from jax import lax
from jax.experimental import pallas as pl
from jax.experimental.pallas import tpu as pltpu
from jax.sharding import PartitionSpec as P

HEAD_DIM = 128
CONV_K = 3
F32 = jnp.float32
BF16 = jnp.bfloat16


def shifted(value, axis, steps):
    count = lax.axis_size(axis)
    leading, last = (max(0, -steps), min(count, count - steps))
    return lax.ppermute(value, axis, [(source, source + steps) for source in range(leading, last)])


def normalize(tokens, norm_gain):
    widened = tokens.astype(jnp.float32)
    inverse = lax.rsqrt(jnp.mean(widened * widened, axis=-1, keepdims=True) + 1e-06)
    return (widened * inverse * norm_gain).astype(jnp.bfloat16)


TILE = 256
NT = (((1,), (1,)), ((), ()))


def softplus(z):
    small = jnp.exp(-jnp.abs(z))
    whole = 1.0 + small
    return jnp.maximum(z, 0.0) + (jnp.log(whole) + (small - (whole - 1.0)))


def attention_kernel(
    q_ref, k_ref, v_ref, shift_ref, later_ref, out_ref, sum_ref, q_split, acc, carry, score, base, after
):
    last = lax.axis_index("sp")
    heads = [pl.ds(0, TILE), pl.ds(TILE, TILE)]
    for h in range(2):
        scaled = q_ref[:, h * HEAD_DIM : (h + 1) * HEAD_DIM].astype(F32) * HEAD_DIM ** (-0.5)
        high = scaled.astype(BF16)
        q_split[heads[h], 0:HEAD_DIM] = high
        q_split[heads[h], HEAD_DIM : 2 * HEAD_DIM] = (scaled - high.astype(F32)).astype(BF16)
    acc[...] = jnp.zeros_like(acc)
    carry[...] = jnp.zeros_like(carry)

    def rows_of(tile):
        return pl.ds(pl.multiple_of(jnp.maximum(tile, 0) * TILE, TILE), TILE)

    def scores(tile, slot):
        key = k_ref[rows_of(tile), :]
        twice = jnp.concatenate([key, key], axis=1)
        for h in range(2):
            score[slot, heads[h], :] = (
                lax.dot_general(q_split[heads[h], :], twice, NT, preferred_element_type=F32)
                + shift_ref[h]
            )

    def sums(slot, masked=False):
        for h in range(2):
            z = score[slot, heads[h], :]
            soft = softplus(z)
            if masked:
                row = lax.broadcasted_iota(jnp.int32, (TILE, TILE), 0)
                col = lax.broadcasted_iota(jnp.int32, (TILE, TILE), 1)
                soft = jnp.where(col < row, soft, 0.0)
                z = jnp.where(col < row, z, -jnp.inf)
            held = carry[heads[h], :]
            base[slot, heads[h], :] = (z - soft) - jnp.concatenate([held, held], axis=1)
            after[slot, heads[h], :] = jnp.dot(
                soft.astype(BF16), later_ref[...], preferred_element_type=F32
            )
            carry[heads[h], :] = held + jnp.sum(soft, axis=1, keepdims=True)

    def weigh(tile, slot):
        value = v_ref[rows_of(tile), :]
        for h in range(2):
            weight = jnp.exp(base[slot, heads[h], :] - after[slot, heads[h], :])
            acc[heads[h], :] += jnp.dot(weight.astype(BF16), value, preferred_element_type=F32)

    scores(last, 0)
    sums(0, True)
    scores(last - 1, 1)

    def two_tiles(step, _):
        tile = last - 1 - 2 * step
        scores(tile - 1, 0)
        sums(1)
        weigh(tile + 1, 0)
        scores(tile - 2, 1)
        sums(0)
        weigh(tile, 1)
        return 0

    lax.fori_loop(0, last // 2, two_tiles, 0)

    @pl.when(last % 2 == 1)
    def _():
        sums(1)
        weigh(1, 0)
        weigh(0, 1)

    @pl.when(last % 2 == 0)
    def _():
        weigh(0, 0)

    for h in range(2):
        out_ref[:, h * HEAD_DIM : (h + 1) * HEAD_DIM] = acc[heads[h], :].astype(BF16)
        sum_ref[:, h * HEAD_DIM : (h + 1) * HEAD_DIM] = carry[heads[h], :]


def attend(queries, key_whole, value_whole, score_shift):
    row_count, width = queries.shape
    later = (jnp.arange(TILE)[:, None] > jnp.arange(TILE)[None, :]).astype(BF16)
    vmem = pl.BlockSpec(memory_space=pltpu.VMEM)
    attended, sums = pl.pallas_call(
        attention_kernel,
        name="attention",
        out_shape=(
            jax.ShapeDtypeStruct((row_count, width), BF16),
            jax.ShapeDtypeStruct((row_count, width), F32),
        ),
        in_specs=[vmem, vmem, vmem, pl.BlockSpec(memory_space=pltpu.SMEM), vmem],
        out_specs=(vmem, vmem),
        scratch_shapes=[
            pltpu.VMEM((2 * TILE, 2 * HEAD_DIM), BF16),
            pltpu.VMEM((2 * TILE, HEAD_DIM), F32),
            pltpu.VMEM((2 * TILE, HEAD_DIM), F32),
            pltpu.VMEM((2, 2 * TILE, TILE), F32),
            pltpu.VMEM((2, 2 * TILE, TILE), F32),
            pltpu.VMEM((2, 2 * TILE, TILE), F32),
        ],
        compiler_params=pltpu.CompilerParams(vmem_limit_bytes=40 * 1024 * 1024),
        cost_estimate=pl.CostEstimate(
            flops=12 * 10**9, bytes_accessed=9 * 10**6, transcendentals=25 * 10**6
        ),
    )(queries, key_whole, value_whole, score_shift, later)
    return attended, sums[:, ::HEAD_DIM]


UP, DOWN, NEXT, BACK, OTHER = range(5)
ZS, YS, CORES = 8, 4, 2


def plan():
    sends = {}
    for dz in range(-3, 5):
        for dy in range(-1, 3):
            first, second = [], []
            if dy == 0:
                if 0 <= dz < 4:
                    first.append((UP, dz + 1, 0))
                if -3 < dz <= 0:
                    first.append((DOWN, dz - 1, 0))
                first += [(NEXT, dz, 1), (BACK, dz, -1)]
            if dy == 1 and dz % 2 == 0:
                first.append((NEXT, dz, 2))
            if dy == -1 and dz % 2 == 1:
                first.append((BACK, dz, 2))
            if dz == 0:
                if dy == 0:
                    second += [(NEXT, 0, 1), (BACK, 0, -1)]
                if dy == 1:
                    second.append((NEXT, 0, 2))
            if 0 <= dz < 3 or (dz == 3 and dy % 2 == 0):
                second.append((UP, dz + 1, dy))
            if -3 < dz <= 0:
                second.append((DOWN, dz - 1, dy))
            if dz == -3 and dy % 2 == 1:
                second.append((DOWN, 4, dy))
            sends[0, dz, dy] = first
            sends[1, dz, dy] = second
    order = sorted(
        (key for key in sends if key[1:] != (0, 0)),
        key=lambda key: (abs(key[1]) + abs(key[2]), abs(key[2]) if key[0] == 0 else abs(key[1]), key),
    )
    return sends, order


def chunk_of(dz, dy):
    return (dz + 3) * YS + dy + 1


class Gather:
    def __init__(self, own, whole, rows, here_sem, side_sem, send_sem):
        self.own, self.whole, self.rows = own, whole, rows
        self.here_sem, self.side_sem, self.send_sem = here_sem, side_sem, send_sem
        sp = lax.axis_index("sp")
        self.z, self.y, self.core = sp // (YS * CORES), (sp // CORES) % YS, sp % CORES
        self.sends, self.order = plan()

    def sp_of(self, z, y, core):
        return (((z + ZS) % ZS) * YS + (y + YS) % YS) * CORES + core

    def neighbour(self, way):
        z, y, core = self.z, self.y, self.core
        return {
            UP: self.sp_of(z + 1, y, core),
            DOWN: self.sp_of(z - 1, y, core),
            NEXT: self.sp_of(z, y + 1, core),
            BACK: self.sp_of(z, y - 1, core),
            OTHER: self.sp_of(z, y, 1 - core),
        }[way]

    def slot(self, half, dz, dy, core):
        origin = self.sp_of(self.z - dz, self.y - dy, core)
        return self.whole[half].at[pl.ds(pl.multiple_of(origin * self.rows, self.rows), self.rows), :]

    def copy(self, half, dz, dy, way, sem):
        dst = self.slot(half, dz, dy, self.core)
        src = self.own[half] if (dz, dy) == (0, 0) else dst
        return pltpu.make_async_remote_copy(
            src_ref=src,
            dst_ref=dst,
            send_sem=self.send_sem.at[half],
            recv_sem=sem,
            device_id={"sp": self.neighbour(way)},
            device_id_type=pl.DeviceIdType.MESH,
        )

    def pass_on(self, half, dz, dy):
        for way, to_dz, to_dy in self.sends[half, dz, dy]:
            self.copy(half, dz, dy, way, self.here_sem.at[half, chunk_of(to_dz % 8 - 8 * (to_dz % 8 > 4), to_dy)]).start()
        self.copy(half, dz, dy, OTHER, self.side_sem.at[half, dz + 3]).start()

    def begin(self):
        for half, ways in ((0, (UP, DOWN)), (1, (NEXT, BACK)), (0, (NEXT, BACK)), (1, (UP, DOWN))):
            for way, to_dz, to_dy in self.sends[half, 0, 0]:
                if way in ways:
                    self.copy(half, 0, 0, way, self.here_sem.at[half, chunk_of(to_dz, to_dy)]).start()
        for half in range(2):
            self.copy(half, 0, 0, OTHER, self.side_sem.at[half, 3]).start()

    def arrive(self, key):
        half, dz, dy = key
        self.copy(half, dz, dy, UP, self.here_sem.at[half, chunk_of(dz, dy)]).wait_recv()
        self.pass_on(half, dz, dy)

    def side(self, half, dz):
        plane = self.whole[half].at[pl.ds(0, YS * self.rows), :]
        pltpu.make_async_copy(plane, plane, self.side_sem.at[half, dz + 3]).wait()

    def finish(self):
        for half in range(2):
            sent = self.whole[half].at[pl.ds(0, (ZS * YS * CORES - 1) * self.rows), :]
            pltpu.make_async_copy(sent, sent, self.send_sem.at[half]).wait()


def greet(gather, around=()):
    barrier = pltpu.get_barrier_semaphore()
    targets = [{"sp": gather.neighbour(way)} for way in (UP, DOWN, NEXT, BACK, OTHER)] + list(around)
    for target in targets:
        pl.semaphore_signal(barrier, inc=1, device_id=target, device_id_type=pl.DeviceIdType.MESH)
    pl.semaphore_wait(barrier, len(targets))


GATHER_SEMS = (
    pltpu.SemaphoreType.DMA((2, ZS * YS)),
    pltpu.SemaphoreType.DMA((2, ZS)),
    pltpu.SemaphoreType.DMA((2,)),
)


def keys_kernel(key_ref, value_ref, key_out, value_out, here_sem, side_sem, send_sem, own_sem):
    gather = Gather((key_ref, value_ref), (key_out, value_out), key_ref.shape[0], here_sem, side_sem, send_sem)
    greet(gather)
    gather.begin()
    kept = [
        pltpu.make_async_copy(gather.own[half], gather.slot(half, 0, 0, gather.core), own_sem.at[half])
        for half in range(2)
    ]
    for copy in kept:
        copy.start()
    for key in gather.order:
        gather.arrive(key)
    for half in range(2):
        for dz in range(-3, 5):
            gather.side(half, dz)
    for copy in kept:
        copy.wait()
    gather.finish()


def gathered_keys(keys, values):
    shape = (keys.shape[0] * ZS * YS * CORES, keys.shape[1])
    vmem = pl.BlockSpec(memory_space=pltpu.VMEM)
    return pl.pallas_call(
        keys_kernel,
        name="gather_keys",
        out_shape=(jax.ShapeDtypeStruct(shape, BF16),) * 2,
        in_specs=[vmem] * 2,
        out_specs=(vmem,) * 2,
        scratch_shapes=[*GATHER_SEMS, pltpu.SemaphoreType.DMA((2,))],
        compiler_params=pltpu.CompilerParams(
            collective_id=1, has_side_effects=True, vmem_limit_bytes=24 * 1024 * 1024
        ),
    )(keys, values)


def tokens_kernel(
    tokens_ref, att_ref, conv_ref, rows_out, att_out, conv_out,
    here_sem, side_sem, send_sem, own_sem, ring_sem, ring_send,
):
    gather = Gather((att_ref, conv_ref), (att_out, conv_out), att_ref.shape[0], here_sem, side_sem, send_sem)
    tp, count = lax.axis_index("tp"), 4
    right, left = {"tp": (tp + 1) % count}, {"tp": (tp + count - 1) % count}
    greet(gather, (right, left))
    rows = tokens_ref.shape[0]
    part = rows // 2

    def piece(origin, at):
        return rows_out.at[pl.ds(pl.multiple_of(((origin + count) % count) * rows + at * part, part), part), :]

    def ring(origin, at, target, number, mine):
        return pltpu.make_async_remote_copy(
            src_ref=tokens_ref.at[pl.ds(at * part, part), :] if mine else piece(origin, at),
            dst_ref=piece(origin, at),
            send_sem=ring_send.at[number],
            recv_sem=ring_sem.at[number],
            device_id=target,
            device_id_type=pl.DeviceIdType.MESH,
        )

    sent = [ring(tp, 0, right, 0, True), ring(tp, 1, left, 2, True), ring(tp, 1, right, 1, True), ring(tp, 0, left, 3, True)]
    for copy in sent:
        copy.start()
    gather.begin()
    kept = [
        pltpu.make_async_copy(gather.own[half], gather.slot(half, 0, 0, gather.core), own_sem.at[half])
        for half in range(2)
    ]
    kept.append(
        pltpu.make_async_copy(tokens_ref, rows_out.at[pl.ds(pl.multiple_of(tp * rows, rows), rows), :], own_sem.at[2])
    )
    for copy in kept:
        copy.start()
    for position, key in enumerate(gather.order):
        if position == 20:
            ring(tp - 1, 0, right, 0, False).wait_recv()
            sent.append(ring(tp - 1, 0, right, 4, False))
            sent[-1].start()
            ring(tp + 1, 1, left, 2, False).wait_recv()
            sent.append(ring(tp + 1, 1, left, 5, False))
            sent[-1].start()
        gather.arrive(key)
    for number, (origin, at) in enumerate(((tp - 1, 1), (tp + 1, 0), (tp - 2, 0), (tp + 2, 1))):
        ring(origin, at, right, (1, 3, 4, 5)[number], False).wait_recv()
    for half in range(2):
        for dz in range(-3, 5):
            gather.side(half, dz)
    for copy in kept:
        copy.wait()
    for copy in sent:
        copy.wait_send()
    gather.finish()


def gathered_rows(tokens, w_out_att, w_out_conv):
    vmem = pl.BlockSpec(memory_space=pltpu.VMEM)
    many = ZS * YS * CORES
    return pl.pallas_call(
        tokens_kernel,
        name="gather_rows",
        out_shape=(
            jax.ShapeDtypeStruct((tokens.shape[0] * 4, tokens.shape[1]), BF16),
            jax.ShapeDtypeStruct((w_out_att.shape[0] * many, w_out_att.shape[1]), BF16),
            jax.ShapeDtypeStruct((w_out_conv.shape[0] * many, w_out_conv.shape[1]), BF16),
        ),
        in_specs=[vmem] * 3,
        out_specs=(vmem,) * 3,
        scratch_shapes=[
            *GATHER_SEMS,
            pltpu.SemaphoreType.DMA((3,)),
            pltpu.SemaphoreType.DMA((6,)),
            pltpu.SemaphoreType.DMA((6,)),
        ],
        compiler_params=pltpu.CompilerParams(
            collective_id=2, has_side_effects=True, vmem_limit_bytes=24 * 1024 * 1024
        ),
    )(tokens, w_out_att, w_out_conv)


def local(
    tokens,
    norm_gain,
    w_query,
    w_key,
    w_value,
    score_shift,
    w_conv_b,
    w_conv_c,
    w_conv_u,
    conv_kernel,
    w_out_att,
    w_out_conv,
):
    weights = (w_query, w_key, w_value, w_conv_b, w_conv_c, w_conv_u)

    def project(rows_in):
        normed = normalize(rows_in, norm_gain)
        return jnp.concatenate(
            [
                jnp.dot(normed, weight, preferred_element_type=jnp.float32).astype(jnp.bfloat16)
                for weight in weights
            ],
            axis=1,
        )

    rows, att_rows, conv_rows = gathered_rows(tokens, w_out_att, w_out_conv)
    projected = project(rows)
    widths = [weight.shape[1] for weight in weights]
    edges = [0]
    for width in widths:
        edges.append(edges[-1] + width)
    queries, keys, values, gate_b, gate_c, inputs_u = [
        projected[:, edges[pos] : edges[pos + 1]] for pos in range(6)
    ]
    tok_count = projected.shape[0]
    conv_local = gate_b.shape[1]
    products = (gate_c.astype(jnp.float32) * inputs_u.astype(jnp.float32)).astype(jnp.bfloat16)
    previous = shifted(products[tok_count - (CONV_K - 1) :], "sp", 1)
    key_whole, value_whole = gathered_keys(keys, values)
    attended, sums_all = attend(queries, key_whole, value_whole, score_shift)
    log_weight = jnp.log(jnp.maximum(-jnp.expm1(-sums_all), 0.05))
    extended = jnp.concatenate([previous, products], axis=0)
    summed = jnp.zeros((tok_count, conv_local), jnp.float32)
    for tap in range(CONV_K):
        summed = summed + conv_kernel[tap][None, :] * extended[tap : tap + tok_count].astype(
            jnp.float32
        )
    convolved = (gate_b.astype(jnp.float32) * summed).astype(jnp.bfloat16)
    contract = (((1,), (1,)), ((), ()))
    share = lax.dot_general(attended, att_rows, contract, preferred_element_type=jnp.float32)
    share = share + lax.dot_general(
        convolved, conv_rows, contract, preferred_element_type=jnp.float32
    )
    rounded = share.astype(jnp.bfloat16).astype(jnp.float32)
    mixed = lax.psum_scatter(rounded.astype(jnp.bfloat16), "tp", scatter_dimension=0, tiled=True)
    return (mixed, log_weight)


def solution(mesh):
    return jax.shard_map(
        local,
        mesh=mesh,
        in_specs=(
            P(("sp", "tp"), None),
            P(),
            P(None, "tp"),
            P(None, "tp"),
            P(None, "tp"),
            P("tp"),
            P(None, "tp"),
            P(None, "tp"),
            P(None, "tp"),
            P(None, "tp"),
            P("sp", "tp"),
            P("sp", "tp"),
        ),
        out_specs=(P(("sp", "tp"), None), P("sp", "tp")),
        check_vma=False,
    )
```

```python
import jax
import jax.numpy as jnp
from jax import lax
from jax.experimental import pallas as pl
from jax.experimental.pallas import tpu as pltpu
from jax.sharding import PartitionSpec as P

HEAD_DIM = 128
CONV_K = 3
F32 = jnp.float32
BF16 = jnp.bfloat16


def shifted(value, axis, steps):
    count = lax.axis_size(axis)
    leading, last = (max(0, -steps), min(count, count - steps))
    return lax.ppermute(value, axis, [(source, source + steps) for source in range(leading, last)])


def normalize(tokens, norm_gain):
    widened = tokens.astype(jnp.float32)
    inverse = lax.rsqrt(jnp.mean(widened * widened, axis=-1, keepdims=True) + 1e-06)
    return (widened * inverse * norm_gain).astype(jnp.bfloat16)


TILE = 256
NT = (((1,), (1,)), ((), ()))


def softplus(z):
    small = jnp.exp(-jnp.abs(z))
    whole = 1.0 + small
    return jnp.maximum(z, 0.0) + (jnp.log(whole) + (small - (whole - 1.0)))


def attention_kernel(
    q_ref, k_ref, v_ref, shift_ref, later_ref, out_ref, sum_ref, q_split, acc, carry, score, base, after
):
    last = lax.axis_index("sp")
    heads = [pl.ds(0, TILE), pl.ds(TILE, TILE)]
    for h in range(2):
        scaled = q_ref[:, h * HEAD_DIM : (h + 1) * HEAD_DIM].astype(F32) * HEAD_DIM ** (-0.5)
        high = scaled.astype(BF16)
        q_split[heads[h], 0:HEAD_DIM] = high
        q_split[heads[h], HEAD_DIM : 2 * HEAD_DIM] = (scaled - high.astype(F32)).astype(BF16)
    acc[...] = jnp.zeros_like(acc)
    carry[...] = jnp.zeros_like(carry)

    def rows_of(tile):
        return pl.ds(pl.multiple_of(jnp.maximum(tile, 0) * TILE, TILE), TILE)

    def scores(tile, slot):
        key = k_ref[rows_of(tile), :]
        twice = jnp.concatenate([key, key], axis=1)
        for h in range(2):
            score[slot, heads[h], :] = (
                lax.dot_general(q_split[heads[h], :], twice, NT, preferred_element_type=F32)
                + shift_ref[h]
            )

    def sums(slot, masked=False):
        for h in range(2):
            z = score[slot, heads[h], :]
            soft = softplus(z)
            if masked:
                row = lax.broadcasted_iota(jnp.int32, (TILE, TILE), 0)
                col = lax.broadcasted_iota(jnp.int32, (TILE, TILE), 1)
                soft = jnp.where(col < row, soft, 0.0)
                z = jnp.where(col < row, z, -jnp.inf)
            held = carry[heads[h], :]
            base[slot, heads[h], :] = (z - soft) - jnp.concatenate([held, held], axis=1)
            after[slot, heads[h], :] = jnp.dot(
                soft.astype(BF16), later_ref[...], preferred_element_type=F32
            )
            carry[heads[h], :] = held + jnp.sum(soft, axis=1, keepdims=True)

    def weigh(tile, slot):
        value = v_ref[rows_of(tile), :]
        for h in range(2):
            weight = jnp.exp(base[slot, heads[h], :] - after[slot, heads[h], :])
            acc[heads[h], :] += jnp.dot(weight.astype(BF16), value, preferred_element_type=F32)

    scores(last, 0)
    sums(0, True)
    scores(last - 1, 1)

    def two_tiles(step, _):
        tile = last - 1 - 2 * step
        scores(tile - 1, 0)
        sums(1)
        weigh(tile + 1, 0)
        scores(tile - 2, 1)
        sums(0)
        weigh(tile, 1)
        return 0

    lax.fori_loop(0, last // 2, two_tiles, 0)

    @pl.when(last % 2 == 1)
    def _():
        sums(1)
        weigh(1, 0)
        weigh(0, 1)

    @pl.when(last % 2 == 0)
    def _():
        weigh(0, 0)

    for h in range(2):
        out_ref[:, h * HEAD_DIM : (h + 1) * HEAD_DIM] = acc[heads[h], :].astype(BF16)
        sum_ref[:, h * HEAD_DIM : (h + 1) * HEAD_DIM] = carry[heads[h], :]


def attend(queries, key_whole, value_whole, score_shift):
    row_count, width = queries.shape
    later = (jnp.arange(TILE)[:, None] > jnp.arange(TILE)[None, :]).astype(BF16)
    vmem = pl.BlockSpec(memory_space=pltpu.VMEM)
    attended, sums = pl.pallas_call(
        attention_kernel,
        name="attention",
        out_shape=(
            jax.ShapeDtypeStruct((row_count, width), BF16),
            jax.ShapeDtypeStruct((row_count, width), F32),
        ),
        in_specs=[vmem, vmem, vmem, pl.BlockSpec(memory_space=pltpu.SMEM), vmem],
        out_specs=(vmem, vmem),
        scratch_shapes=[
            pltpu.VMEM((2 * TILE, 2 * HEAD_DIM), BF16),
            pltpu.VMEM((2 * TILE, HEAD_DIM), F32),
            pltpu.VMEM((2 * TILE, HEAD_DIM), F32),
            pltpu.VMEM((2, 2 * TILE, TILE), F32),
            pltpu.VMEM((2, 2 * TILE, TILE), F32),
            pltpu.VMEM((2, 2 * TILE, TILE), F32),
        ],
        compiler_params=pltpu.CompilerParams(vmem_limit_bytes=40 * 1024 * 1024),
        cost_estimate=pl.CostEstimate(
            flops=12 * 10**9, bytes_accessed=9 * 10**6, transcendentals=25 * 10**6
        ),
    )(queries, key_whole, value_whole, score_shift, later)
    return attended, sums[:, ::HEAD_DIM]


UP, DOWN, NEXT, BACK, OTHER = range(5)
ZS, YS, CORES = 8, 4, 2


def plan():
    sends = {}
    for dz in range(-3, 5):
        for dy in range(-1, 3):
            first, second = [], []
            if dy == 0:
                if 0 <= dz < 4:
                    first.append((UP, dz + 1, 0))
                if -3 < dz <= 0:
                    first.append((DOWN, dz - 1, 0))
                first += [(NEXT, dz, 1), (BACK, dz, -1)]
            if dy == 1 and dz % 2 == 0:
                first.append((NEXT, dz, 2))
            if dy == -1 and dz % 2 == 1:
                first.append((BACK, dz, 2))
            if dz == 0:
                if dy == 0:
                    second += [(NEXT, 0, 1), (BACK, 0, -1)]
                if dy == 1:
                    second.append((NEXT, 0, 2))
            if 0 <= dz < 3 or (dz == 3 and dy % 2 == 0):
                second.append((UP, dz + 1, dy))
            if -3 < dz <= 0:
                second.append((DOWN, dz - 1, dy))
            if dz == -3 and dy % 2 == 1:
                second.append((DOWN, 4, dy))
            sends[0, dz, dy] = first
            sends[1, dz, dy] = second
    order = sorted(
        (key for key in sends if key[1:] != (0, 0)),
        key=lambda key: (abs(key[1]) + abs(key[2]), abs(key[2]) if key[0] == 0 else abs(key[1]), key),
    )
    return sends, order


def chunk_of(dz, dy):
    return (dz + 3) * YS + dy + 1


class Gather:
    def __init__(self, own, whole, rows, here_sem, side_sem, send_sem):
        self.own, self.whole, self.rows = own, whole, rows
        self.here_sem, self.side_sem, self.send_sem = here_sem, side_sem, send_sem
        sp = lax.axis_index("sp")
        self.z, self.y, self.core = sp // (YS * CORES), (sp // CORES) % YS, sp % CORES
        self.sends, self.order = plan()

    def sp_of(self, z, y, core):
        return (((z + ZS) % ZS) * YS + (y + YS) % YS) * CORES + core

    def neighbour(self, way):
        z, y, core = self.z, self.y, self.core
        return {
            UP: self.sp_of(z + 1, y, core),
            DOWN: self.sp_of(z - 1, y, core),
            NEXT: self.sp_of(z, y + 1, core),
            BACK: self.sp_of(z, y - 1, core),
            OTHER: self.sp_of(z, y, 1 - core),
        }[way]

    def slot(self, half, dz, dy, core):
        origin = self.sp_of(self.z - dz, self.y - dy, core)
        return self.whole[half].at[pl.ds(pl.multiple_of(origin * self.rows, self.rows), self.rows), :]

    def copy(self, half, dz, dy, way, sem):
        dst = self.slot(half, dz, dy, self.core)
        src = self.own[half] if (dz, dy) == (0, 0) else dst
        return pltpu.make_async_remote_copy(
            src_ref=src,
            dst_ref=dst,
            send_sem=self.send_sem.at[half],
            recv_sem=sem,
            device_id={"sp": self.neighbour(way)},
            device_id_type=pl.DeviceIdType.MESH,
        )

    def pass_on(self, half, dz, dy):
        for way, to_dz, to_dy in self.sends[half, dz, dy]:
            self.copy(half, dz, dy, way, self.here_sem.at[half, chunk_of(to_dz % 8 - 8 * (to_dz % 8 > 4), to_dy)]).start()
        self.copy(half, dz, dy, OTHER, self.side_sem.at[half, dz + 3]).start()

    def begin(self):
        for half, ways in ((0, (UP, DOWN)), (1, (NEXT, BACK)), (0, (NEXT, BACK)), (1, (UP, DOWN))):
            for way, to_dz, to_dy in self.sends[half, 0, 0]:
                if way in ways:
                    self.copy(half, 0, 0, way, self.here_sem.at[half, chunk_of(to_dz, to_dy)]).start()
        for half in range(2):
            self.copy(half, 0, 0, OTHER, self.side_sem.at[half, 3]).start()

    def arrive(self, key):
        half, dz, dy = key
        self.copy(half, dz, dy, UP, self.here_sem.at[half, chunk_of(dz, dy)]).wait_recv()
        self.pass_on(half, dz, dy)

    def side(self, half, dz):
        plane = self.whole[half].at[pl.ds(0, YS * self.rows), :]
        pltpu.make_async_copy(plane, plane, self.side_sem.at[half, dz + 3]).wait()

    def finish(self):
        for half in range(2):
            sent = self.whole[half].at[pl.ds(0, (ZS * YS * CORES - 1) * self.rows), :]
            pltpu.make_async_copy(sent, sent, self.send_sem.at[half]).wait()


def greet(gather, around=()):
    barrier = pltpu.get_barrier_semaphore()
    targets = [{"sp": gather.neighbour(way)} for way in (UP, DOWN, NEXT, BACK, OTHER)] + list(around)
    for target in targets:
        pl.semaphore_signal(barrier, inc=1, device_id=target, device_id_type=pl.DeviceIdType.MESH)
    pl.semaphore_wait(barrier, len(targets))


GATHER_SEMS = (
    pltpu.SemaphoreType.DMA((2, ZS * YS)),
    pltpu.SemaphoreType.DMA((2, ZS)),
    pltpu.SemaphoreType.DMA((2,)),
)


def keys_kernel(key_ref, value_ref, key_out, value_out, here_sem, side_sem, send_sem, own_sem):
    gather = Gather((key_ref, value_ref), (key_out, value_out), key_ref.shape[0], here_sem, side_sem, send_sem)
    greet(gather)
    gather.begin()
    kept = [
        pltpu.make_async_copy(gather.own[half], gather.slot(half, 0, 0, gather.core), own_sem.at[half])
        for half in range(2)
    ]
    for copy in kept:
        copy.start()
    for key in gather.order:
        gather.arrive(key)
    for half in range(2):
        for dz in range(-3, 5):
            gather.side(half, dz)
    for copy in kept:
        copy.wait()
    gather.finish()


def gathered_keys(keys, values):
    shape = (keys.shape[0] * ZS * YS * CORES, keys.shape[1])
    vmem = pl.BlockSpec(memory_space=pltpu.VMEM)
    return pl.pallas_call(
        keys_kernel,
        name="gather_keys",
        out_shape=(jax.ShapeDtypeStruct(shape, BF16),) * 2,
        in_specs=[vmem] * 2,
        out_specs=(vmem,) * 2,
        scratch_shapes=[*GATHER_SEMS, pltpu.SemaphoreType.DMA((2,))],
        compiler_params=pltpu.CompilerParams(
            collective_id=1, has_side_effects=True, vmem_limit_bytes=24 * 1024 * 1024
        ),
    )(keys, values)


def tokens_kernel(
    tokens_ref, att_ref, conv_ref, rows_out, att_out, conv_out,
    here_sem, side_sem, send_sem, own_sem, ring_sem, ring_send,
):
    gather = Gather((att_ref, conv_ref), (att_out, conv_out), att_ref.shape[0], here_sem, side_sem, send_sem)
    tp, count = lax.axis_index("tp"), 4
    right, left = {"tp": (tp + 1) % count}, {"tp": (tp + count - 1) % count}
    greet(gather, (right, left))
    rows = tokens_ref.shape[0]
    part = rows // 2

    def piece(origin, at):
        return rows_out.at[pl.ds(pl.multiple_of(((origin + count) % count) * rows + at * part, part), part), :]

    def ring(origin, at, target, number, mine):
        return pltpu.make_async_remote_copy(
            src_ref=tokens_ref.at[pl.ds(at * part, part), :] if mine else piece(origin, at),
            dst_ref=piece(origin, at),
            send_sem=ring_send.at[number],
            recv_sem=ring_sem.at[number],
            device_id=target,
            device_id_type=pl.DeviceIdType.MESH,
        )

    sent = [ring(tp, 0, right, 0, True), ring(tp, 1, left, 2, True), ring(tp, 1, right, 1, True), ring(tp, 0, left, 3, True)]
    for copy in sent:
        copy.start()
    gather.begin()
    kept = [
        pltpu.make_async_copy(gather.own[half], gather.slot(half, 0, 0, gather.core), own_sem.at[half])
        for half in range(2)
    ]
    kept.append(
        pltpu.make_async_copy(tokens_ref, rows_out.at[pl.ds(pl.multiple_of(tp * rows, rows), rows), :], own_sem.at[2])
    )
    for copy in kept:
        copy.start()
    for position, key in enumerate(gather.order):
        if position == 20:
            ring(tp - 1, 0, right, 0, False).wait_recv()
            sent.append(ring(tp - 1, 0, right, 4, False))
            sent[-1].start()
            ring(tp + 1, 1, left, 2, False).wait_recv()
            sent.append(ring(tp + 1, 1, left, 5, False))
            sent[-1].start()
        gather.arrive(key)
    for number, (origin, at) in enumerate(((tp - 1, 1), (tp + 1, 0), (tp - 2, 0), (tp + 2, 1))):
        ring(origin, at, right, (1, 3, 4, 5)[number], False).wait_recv()
    for half in range(2):
        for dz in range(-3, 5):
            gather.side(half, dz)
    for copy in kept:
        copy.wait()
    for copy in sent:
        copy.wait_send()
    gather.finish()


def gathered_rows(tokens, w_out_att, w_out_conv):
    vmem = pl.BlockSpec(memory_space=pltpu.VMEM)
    many = ZS * YS * CORES
    return pl.pallas_call(
        tokens_kernel,
        name="gather_rows",
        out_shape=(
            jax.ShapeDtypeStruct((tokens.shape[0] * 4, tokens.shape[1]), BF16),
            jax.ShapeDtypeStruct((w_out_att.shape[0] * many, w_out_att.shape[1]), BF16),
            jax.ShapeDtypeStruct((w_out_conv.shape[0] * many, w_out_conv.shape[1]), BF16),
        ),
        in_specs=[vmem] * 3,
        out_specs=(vmem,) * 3,
        scratch_shapes=[
            *GATHER_SEMS,
            pltpu.SemaphoreType.DMA((3,)),
            pltpu.SemaphoreType.DMA((6,)),
            pltpu.SemaphoreType.DMA((6,)),
        ],
        compiler_params=pltpu.CompilerParams(
            collective_id=2, has_side_effects=True, vmem_limit_bytes=24 * 1024 * 1024
        ),
    )(tokens, w_out_att, w_out_conv)


OUT_BLOCKS = 8
BLOCK_ORDER = (0, 4, 1, 5, 2, 6, 3, 7)


def output_kernel(
    att_ref, conv_ref, att_rows, conv_rows, out_ref, share, from_left, from_right, passing, passed,
    share_send, passed_send, left_sem, right_sem, passing_sem,
):
    tp, count = lax.axis_index("tp"), 4
    right, left = (tp + 1) % count, (tp + count - 1) % count
    across = (tp + 2) % count
    barrier = pltpu.get_barrier_semaphore()
    for target in (left, right):
        pl.semaphore_signal(barrier, inc=1, device_id={"tp": target}, device_id_type=pl.DeviceIdType.MESH)
    pl.semaphore_wait(barrier, 2)
    rows = out_ref.shape[0]
    width = out_ref.shape[1] // OUT_BLOCKS
    half = OUT_BLOCKS // 2

    def columns(block):
        return pl.ds(block * width, width)

    def rows_for(target):
        return pl.ds(pl.multiple_of(target * rows, rows), rows)

    def remote(src, dst, send, recv, target):
        return pltpu.make_async_remote_copy(
            src_ref=src, dst_ref=dst, send_sem=send, recv_sem=recv,
            device_id={"tp": target}, device_id_type=pl.DeviceIdType.MESH,
        )

    def onward(block):
        low = block < half
        return remote(
            share.at[rows_for(across), columns(block)], passing.at[:, columns(block)],
            share_send.at[0, block], passing_sem.at[block], left if low else right,
        )

    def direct(block):
        low = block < half
        return remote(
            share.at[rows_for(right if low else left), columns(block)],
            (from_left if low else from_right).at[:, columns(block)],
            share_send.at[1, block], (left_sem if low else right_sem).at[block], right if low else left,
        )

    def summed(block):
        low = block < half
        return remote(
            passed.at[:, columns(block)], (from_right if low else from_left).at[:, columns(block)],
            passed_send.at[block], (right_sem if low else left_sem).at[block], left if low else right,
        )

    for block in BLOCK_ORDER:
        part = lax.dot_general(att_ref[...], att_rows[columns(block), :], NT, preferred_element_type=F32)
        part = part + lax.dot_general(conv_ref[...], conv_rows[columns(block), :], NT, preferred_element_type=F32)
        share[:, columns(block)] = part.astype(BF16)
        onward(block).start()
        direct(block).start()
    for block in BLOCK_ORDER:
        onward(block).wait_recv()
        mine = share[rows_for(left if block < half else right), columns(block)]
        passed[:, columns(block)] = (mine.astype(F32) + passing[:, columns(block)].astype(F32)).astype(BF16)
        summed(block).start()
    for block in BLOCK_ORDER:
        direct(block).wait_recv()
        summed(block).wait_recv()
        total = share[rows_for(tp), columns(block)].astype(F32) + from_left[:, columns(block)].astype(F32)
        out_ref[:, columns(block)] = (total + from_right[:, columns(block)].astype(F32)).astype(BF16)
    for block in range(OUT_BLOCKS):
        onward(block).wait_send()
        direct(block).wait_send()
        summed(block).wait_send()


def mixed_rows(attended, convolved, att_rows, conv_rows):
    count, features = attended.shape[0], att_rows.shape[0]
    rows = count // 4
    vmem = pl.BlockSpec(memory_space=pltpu.VMEM)
    slab = pltpu.VMEM((rows, features), BF16)
    sems = pltpu.SemaphoreType.DMA((OUT_BLOCKS,))
    return pl.pallas_call(
        output_kernel,
        name="output",
        out_shape=jax.ShapeDtypeStruct((rows, features), BF16),
        in_specs=[vmem] * 4,
        out_specs=vmem,
        scratch_shapes=[
            pltpu.VMEM((count, features), BF16), slab, slab, slab, slab,
            pltpu.SemaphoreType.DMA((2, OUT_BLOCKS)), sems, sems, sems, sems,
        ],
        compiler_params=pltpu.CompilerParams(
            collective_id=3, has_side_effects=True, vmem_limit_bytes=24 * 1024 * 1024
        ),
    )(attended, convolved, att_rows, conv_rows)


def local(
    tokens,
    norm_gain,
    w_query,
    w_key,
    w_value,
    score_shift,
    w_conv_b,
    w_conv_c,
    w_conv_u,
    conv_kernel,
    w_out_att,
    w_out_conv,
):
    weights = (w_query, w_key, w_value, w_conv_b, w_conv_c, w_conv_u)

    def project(rows_in):
        normed = normalize(rows_in, norm_gain)
        return jnp.concatenate(
            [
                jnp.dot(normed, weight, preferred_element_type=jnp.float32).astype(jnp.bfloat16)
                for weight in weights
            ],
            axis=1,
        )

    rows, att_rows, conv_rows = gathered_rows(tokens, w_out_att, w_out_conv)
    projected = project(rows)
    widths = [weight.shape[1] for weight in weights]
    edges = [0]
    for width in widths:
        edges.append(edges[-1] + width)
    queries, keys, values, gate_b, gate_c, inputs_u = [
        projected[:, edges[pos] : edges[pos + 1]] for pos in range(6)
    ]
    tok_count = projected.shape[0]
    conv_local = gate_b.shape[1]
    products = (gate_c.astype(jnp.float32) * inputs_u.astype(jnp.float32)).astype(jnp.bfloat16)
    previous = shifted(products[tok_count - (CONV_K - 1) :], "sp", 1)
    key_whole, value_whole = gathered_keys(keys, values)
    attended, sums_all = attend(queries, key_whole, value_whole, score_shift)
    log_weight = jnp.log(jnp.maximum(-jnp.expm1(-sums_all), 0.05))
    extended = jnp.concatenate([previous, products], axis=0)
    summed = jnp.zeros((tok_count, conv_local), jnp.float32)
    for tap in range(CONV_K):
        summed = summed + conv_kernel[tap][None, :] * extended[tap : tap + tok_count].astype(
            jnp.float32
        )
    convolved = (gate_b.astype(jnp.float32) * summed).astype(jnp.bfloat16)
    mixed = mixed_rows(attended, convolved, att_rows, conv_rows)
    return (mixed, log_weight)


def solution(mesh):
    return jax.shard_map(
        local,
        mesh=mesh,
        in_specs=(
            P(("sp", "tp"), None),
            P(),
            P(None, "tp"),
            P(None, "tp"),
            P(None, "tp"),
            P("tp"),
            P(None, "tp"),
            P(None, "tp"),
            P(None, "tp"),
            P(None, "tp"),
            P("sp", "tp"),
            P("sp", "tp"),
        ),
        out_specs=(P(("sp", "tp"), None), P("sp", "tp")),
        check_vma=False,
    )
```

```python
import jax
import jax.numpy as jnp
from jax import lax
from jax.experimental import pallas as pl
from jax.experimental.pallas import tpu as pltpu
from jax.sharding import PartitionSpec as P

HEAD_DIM = 128
CONV_K = 3
F32 = jnp.float32
BF16 = jnp.bfloat16


def shifted(value, axis, steps):
    count = lax.axis_size(axis)
    leading, last = (max(0, -steps), min(count, count - steps))
    return lax.ppermute(value, axis, [(source, source + steps) for source in range(leading, last)])


def normalize(tokens, norm_gain):
    widened = tokens.astype(jnp.float32)
    inverse = lax.rsqrt(jnp.mean(widened * widened, axis=-1, keepdims=True) + 1e-06)
    return (widened * inverse * norm_gain).astype(jnp.bfloat16)


TILE = 256
NT = (((1,), (1,)), ((), ()))


def softplus(z):
    small = jnp.exp(-jnp.abs(z))
    whole = 1.0 + small
    return jnp.maximum(z, 0.0) + (jnp.log(whole) + (small - (whole - 1.0)))


def attention_kernel(
    q_ref, k_ref, v_ref, shift_ref, later_ref, out_ref, sum_ref, q_split, acc, carry, score, base, after
):
    last = lax.axis_index("sp")
    heads = [pl.ds(0, TILE), pl.ds(TILE, TILE)]
    for h in range(2):
        scaled = q_ref[:, h * HEAD_DIM : (h + 1) * HEAD_DIM].astype(F32) * HEAD_DIM ** (-0.5)
        high = scaled.astype(BF16)
        q_split[heads[h], 0:HEAD_DIM] = high
        q_split[heads[h], HEAD_DIM : 2 * HEAD_DIM] = (scaled - high.astype(F32)).astype(BF16)
    acc[...] = jnp.zeros_like(acc)
    carry[...] = jnp.zeros_like(carry)

    def rows_of(tile):
        return pl.ds(pl.multiple_of(jnp.maximum(tile, 0) * TILE, TILE), TILE)

    def scores(tile, slot):
        key = k_ref[rows_of(tile), :]
        twice = jnp.concatenate([key, key], axis=1)
        for h in range(2):
            score[slot, heads[h], :] = (
                lax.dot_general(q_split[heads[h], :], twice, NT, preferred_element_type=F32)
                + shift_ref[h]
            )

    def sums(slot, masked=False):
        for h in range(2):
            z = score[slot, heads[h], :]
            soft = softplus(z)
            if masked:
                row = lax.broadcasted_iota(jnp.int32, (TILE, TILE), 0)
                col = lax.broadcasted_iota(jnp.int32, (TILE, TILE), 1)
                soft = jnp.where(col < row, soft, 0.0)
                z = jnp.where(col < row, z, -jnp.inf)
            held = carry[heads[h], :]
            base[slot, heads[h], :] = (z - soft) - jnp.concatenate([held, held], axis=1)
            after[slot, heads[h], :] = jnp.dot(
                soft.astype(BF16), later_ref[...], preferred_element_type=F32
            )
            carry[heads[h], :] = held + jnp.sum(soft, axis=1, keepdims=True)

    def weigh(tile, slot):
        value = v_ref[rows_of(tile), :]
        for h in range(2):
            weight = jnp.exp(base[slot, heads[h], :] - after[slot, heads[h], :])
            acc[heads[h], :] += jnp.dot(weight.astype(BF16), value, preferred_element_type=F32)

    scores(last, 0)
    sums(0, True)
    scores(last - 1, 1)

    def two_tiles(step, _):
        tile = last - 1 - 2 * step
        scores(tile - 1, 0)
        sums(1)
        weigh(tile + 1, 0)
        scores(tile - 2, 1)
        sums(0)
        weigh(tile, 1)
        return 0

    lax.fori_loop(0, last // 2, two_tiles, 0)

    @pl.when(last % 2 == 1)
    def _():
        sums(1)
        weigh(1, 0)
        weigh(0, 1)

    @pl.when(last % 2 == 0)
    def _():
        weigh(0, 0)

    for h in range(2):
        out_ref[:, h * HEAD_DIM : (h + 1) * HEAD_DIM] = acc[heads[h], :].astype(BF16)
        sum_ref[h : h + 1, :] = jnp.transpose(carry[heads[h], :])[0:1, :]


def attend(queries, key_whole, value_whole, score_shift):
    row_count, width = queries.shape
    later = (jnp.arange(TILE)[:, None] > jnp.arange(TILE)[None, :]).astype(BF16)
    vmem = pl.BlockSpec(memory_space=pltpu.VMEM)
    attended, sums = pl.pallas_call(
        attention_kernel,
        name="attention",
        out_shape=(
            jax.ShapeDtypeStruct((row_count, width), BF16),
            jax.ShapeDtypeStruct((2, row_count), F32),
        ),
        in_specs=[vmem, vmem, vmem, pl.BlockSpec(memory_space=pltpu.SMEM), vmem],
        out_specs=(vmem, vmem),
        scratch_shapes=[
            pltpu.VMEM((2 * TILE, 2 * HEAD_DIM), BF16),
            pltpu.VMEM((2 * TILE, HEAD_DIM), F32),
            pltpu.VMEM((2 * TILE, HEAD_DIM), F32),
            pltpu.VMEM((2, 2 * TILE, TILE), F32),
            pltpu.VMEM((2, 2 * TILE, TILE), F32),
            pltpu.VMEM((2, 2 * TILE, TILE), F32),
        ],
        compiler_params=pltpu.CompilerParams(vmem_limit_bytes=16 * 1024 * 1024),
        cost_estimate=pl.CostEstimate(
            flops=12 * 10**9, bytes_accessed=9 * 10**6, transcendentals=25 * 10**6
        ),
    )(queries, key_whole, value_whole, score_shift, later)
    return attended, sums


UP, DOWN, NEXT, BACK, OTHER = range(5)
ZS, YS, CORES = 8, 4, 2


def plan():
    sends = {}
    for dz in range(-3, 5):
        for dy in range(-1, 3):
            first, second = [], []
            if dy == 0:
                if 0 <= dz < 4:
                    first.append((UP, dz + 1, 0))
                if -3 < dz <= 0:
                    first.append((DOWN, dz - 1, 0))
                first += [(NEXT, dz, 1), (BACK, dz, -1)]
            if dy == 1 and dz % 2 == 0:
                first.append((NEXT, dz, 2))
            if dy == -1 and dz % 2 == 1:
                first.append((BACK, dz, 2))
            if dz == 0:
                if dy == 0:
                    second += [(NEXT, 0, 1), (BACK, 0, -1)]
                if dy == 1:
                    second.append((NEXT, 0, 2))
            if 0 <= dz < 3 or (dz == 3 and dy % 2 == 0):
                second.append((UP, dz + 1, dy))
            if -3 < dz <= 0:
                second.append((DOWN, dz - 1, dy))
            if dz == -3 and dy % 2 == 1:
                second.append((DOWN, 4, dy))
            sends[0, dz, dy] = first
            sends[1, dz, dy] = second
    order = sorted(
        (key for key in sends if key[1:] != (0, 0)),
        key=lambda key: (abs(key[1]) + abs(key[2]), abs(key[2]) if key[0] == 0 else abs(key[1]), key),
    )
    return sends, order


def chunk_of(dz, dy):
    return (dz + 3) * YS + dy + 1


class Gather:
    def __init__(self, own, whole, rows, here_sem, side_sem, send_sem):
        self.own, self.whole, self.rows = own, whole, rows
        self.here_sem, self.side_sem, self.send_sem = here_sem, side_sem, send_sem
        sp = lax.axis_index("sp")
        self.z, self.y, self.core = sp // (YS * CORES), (sp // CORES) % YS, sp % CORES
        self.sends, self.order = plan()

    def sp_of(self, z, y, core):
        return (((z + ZS) % ZS) * YS + (y + YS) % YS) * CORES + core

    def neighbour(self, way):
        z, y, core = self.z, self.y, self.core
        return {
            UP: self.sp_of(z + 1, y, core),
            DOWN: self.sp_of(z - 1, y, core),
            NEXT: self.sp_of(z, y + 1, core),
            BACK: self.sp_of(z, y - 1, core),
            OTHER: self.sp_of(z, y, 1 - core),
        }[way]

    def slot(self, half, dz, dy, core):
        origin = self.sp_of(self.z - dz, self.y - dy, core)
        return self.whole[half].at[pl.ds(pl.multiple_of(origin * self.rows, self.rows), self.rows), :]

    def copy(self, half, dz, dy, way, sem):
        dst = self.slot(half, dz, dy, self.core)
        src = self.own[half] if (dz, dy) == (0, 0) else dst
        return pltpu.make_async_remote_copy(
            src_ref=src,
            dst_ref=dst,
            send_sem=self.send_sem.at[half],
            recv_sem=sem,
            device_id={"sp": self.neighbour(way)},
            device_id_type=pl.DeviceIdType.MESH,
        )

    def pass_on(self, half, dz, dy):
        for way, to_dz, to_dy in self.sends[half, dz, dy]:
            self.copy(half, dz, dy, way, self.here_sem.at[half, chunk_of(to_dz % 8 - 8 * (to_dz % 8 > 4), to_dy)]).start()
        self.copy(half, dz, dy, OTHER, self.side_sem.at[half, dz + 3]).start()

    def begin(self):
        for half, ways in ((0, (UP, DOWN)), (1, (NEXT, BACK)), (0, (NEXT, BACK)), (1, (UP, DOWN))):
            for way, to_dz, to_dy in self.sends[half, 0, 0]:
                if way in ways:
                    self.copy(half, 0, 0, way, self.here_sem.at[half, chunk_of(to_dz, to_dy)]).start()
        for half in range(2):
            self.copy(half, 0, 0, OTHER, self.side_sem.at[half, 3]).start()

    def arrive(self, key):
        half, dz, dy = key
        self.copy(half, dz, dy, UP, self.here_sem.at[half, chunk_of(dz, dy)]).wait_recv()
        self.pass_on(half, dz, dy)

    def side(self, half, dz):
        plane = self.whole[half].at[pl.ds(0, YS * self.rows), :]
        pltpu.make_async_copy(plane, plane, self.side_sem.at[half, dz + 3]).wait()

    def finish(self):
        for half in range(2):
            sent = self.whole[half].at[pl.ds(0, (ZS * YS * CORES - 1) * self.rows), :]
            pltpu.make_async_copy(sent, sent, self.send_sem.at[half]).wait()


def greet(gather, around=()):
    barrier = pltpu.get_barrier_semaphore()
    targets = [{"sp": gather.neighbour(way)} for way in (UP, DOWN, NEXT, BACK, OTHER)] + list(around)
    for target in targets:
        pl.semaphore_signal(barrier, inc=1, device_id=target, device_id_type=pl.DeviceIdType.MESH)
    pl.semaphore_wait(barrier, len(targets))


GATHER_SEMS = (
    pltpu.SemaphoreType.DMA((2, ZS * YS)),
    pltpu.SemaphoreType.DMA((2, ZS)),
    pltpu.SemaphoreType.DMA((2,)),
)


PROJECT_AFTER = (8, 16, 24, 32)


def keys_kernel(
    key_ref, value_ref, normed_ref, wq_ref, wb_ref, wc_ref, wu_ref,
    key_out, value_out, query_out, gate_b_out, gate_c_out, input_out,
    here_sem, side_sem, send_sem, own_sem,
):
    gather = Gather((key_ref, value_ref), (key_out, value_out), key_ref.shape[0], here_sem, side_sem, send_sem)
    weights = (wq_ref, wb_ref, wc_ref, wu_ref)
    greet(gather)
    gather.begin()
    kept = [
        pltpu.make_async_copy(gather.own[half], gather.slot(half, 0, 0, gather.core), own_sem.at[half])
        for half in range(2)
    ]
    for copy in kept:
        copy.start()
    outs = (query_out, gate_b_out, gate_c_out, input_out)
    for position, key in enumerate(gather.order):
        if position in PROJECT_AFTER:
            number = PROJECT_AFTER.index(position)
            outs[number][...] = jnp.dot(
                normed_ref[...], weights[number][...], preferred_element_type=F32
            ).astype(BF16)
        gather.arrive(key)
    for half in range(2):
        for dz in range(-3, 5):
            gather.side(half, dz)
    for copy in kept:
        copy.wait()
    gather.finish()


def gathered_keys(keys, values, normed, weights):
    shape = (keys.shape[0] * ZS * YS * CORES, keys.shape[1])
    vmem = pl.BlockSpec(memory_space=pltpu.VMEM)
    projected = jax.ShapeDtypeStruct((normed.shape[0], weights[0].shape[1]), BF16)
    return pl.pallas_call(
        keys_kernel,
        name="gather_keys",
        out_shape=(jax.ShapeDtypeStruct(shape, BF16),) * 2 + (projected,) * 4,
        in_specs=[vmem] * 7,
        out_specs=(vmem,) * 6,
        scratch_shapes=[
            *GATHER_SEMS,
            pltpu.SemaphoreType.DMA((2,)),
        ],
        compiler_params=pltpu.CompilerParams(
            collective_id=1, has_side_effects=True, vmem_limit_bytes=24 * 1024 * 1024
        ),
    )(keys, values, normed, *weights)


def tokens_kernel(
    tokens_ref, att_ref, conv_ref, rows_out, att_out, conv_out,
    here_sem, side_sem, send_sem, own_sem, ring_sem, ring_send,
):
    gather = Gather((att_ref, conv_ref), (att_out, conv_out), att_ref.shape[0], here_sem, side_sem, send_sem)
    tp, count = lax.axis_index("tp"), 4
    right, left = {"tp": (tp + 1) % count}, {"tp": (tp + count - 1) % count}
    greet(gather, (right, left))
    rows = tokens_ref.shape[0]
    part = rows // 2

    def piece(origin, at):
        return rows_out.at[pl.ds(pl.multiple_of(((origin + count) % count) * rows + at * part, part), part), :]

    def ring(origin, at, target, number, mine):
        return pltpu.make_async_remote_copy(
            src_ref=tokens_ref.at[pl.ds(at * part, part), :] if mine else piece(origin, at),
            dst_ref=piece(origin, at),
            send_sem=ring_send.at[number],
            recv_sem=ring_sem.at[number],
            device_id=target,
            device_id_type=pl.DeviceIdType.MESH,
        )

    sent = [ring(tp, 0, right, 0, True), ring(tp, 1, left, 2, True), ring(tp, 1, right, 1, True), ring(tp, 0, left, 3, True)]
    for copy in sent:
        copy.start()
    gather.begin()
    kept = [
        pltpu.make_async_copy(gather.own[half], gather.slot(half, 0, 0, gather.core), own_sem.at[half])
        for half in range(2)
    ]
    kept.append(
        pltpu.make_async_copy(tokens_ref, rows_out.at[pl.ds(pl.multiple_of(tp * rows, rows), rows), :], own_sem.at[2])
    )
    for copy in kept:
        copy.start()
    for position, key in enumerate(gather.order):
        if position == 20:
            ring(tp - 1, 0, right, 0, False).wait_recv()
            sent.append(ring(tp - 1, 0, right, 4, False))
            sent[-1].start()
            ring(tp + 1, 1, left, 2, False).wait_recv()
            sent.append(ring(tp + 1, 1, left, 5, False))
            sent[-1].start()
        gather.arrive(key)
    for number, (origin, at) in enumerate(((tp - 1, 1), (tp + 1, 0), (tp - 2, 0), (tp + 2, 1))):
        ring(origin, at, right, (1, 3, 4, 5)[number], False).wait_recv()
    for half in range(2):
        for dz in range(-3, 5):
            gather.side(half, dz)
    for copy in kept:
        copy.wait()
    for copy in sent:
        copy.wait_send()
    gather.finish()


def gathered_rows(tokens, w_out_att, w_out_conv):
    vmem = pl.BlockSpec(memory_space=pltpu.VMEM)
    many = ZS * YS * CORES
    return pl.pallas_call(
        tokens_kernel,
        name="gather_rows",
        out_shape=(
            jax.ShapeDtypeStruct((tokens.shape[0] * 4, tokens.shape[1]), BF16),
            jax.ShapeDtypeStruct((w_out_att.shape[0] * many, w_out_att.shape[1]), BF16),
            jax.ShapeDtypeStruct((w_out_conv.shape[0] * many, w_out_conv.shape[1]), BF16),
        ),
        in_specs=[pl.BlockSpec(memory_space=pltpu.HBM)] * 3,
        out_specs=(vmem,) * 3,
        scratch_shapes=[
            *GATHER_SEMS,
            pltpu.SemaphoreType.DMA((3,)),
            pltpu.SemaphoreType.DMA((6,)),
            pltpu.SemaphoreType.DMA((6,)),
        ],
        compiler_params=pltpu.CompilerParams(
            collective_id=2, has_side_effects=True, vmem_limit_bytes=24 * 1024 * 1024
        ),
    )(tokens, w_out_att, w_out_conv)


OUT_BLOCKS = 8
BLOCK_ORDER = (0, 4, 1, 5, 2, 6, 3, 7)


def output_kernel(
    att_ref, conv_ref, att_rows, conv_rows, out_ref, share, from_left, from_right, passing, passed,
    share_send, passed_send, left_sem, right_sem, passing_sem,
):
    tp, count = lax.axis_index("tp"), 4
    right, left = (tp + 1) % count, (tp + count - 1) % count
    across = (tp + 2) % count
    barrier = pltpu.get_barrier_semaphore()
    for target in (left, right):
        pl.semaphore_signal(barrier, inc=1, device_id={"tp": target}, device_id_type=pl.DeviceIdType.MESH)
    pl.semaphore_wait(barrier, 2)
    rows = out_ref.shape[0]
    width = out_ref.shape[1] // OUT_BLOCKS
    half = OUT_BLOCKS // 2

    def columns(block):
        return pl.ds(block * width, width)

    def rows_for(target):
        return pl.ds(pl.multiple_of(target * rows, rows), rows)

    def remote(src, dst, send, recv, target):
        return pltpu.make_async_remote_copy(
            src_ref=src, dst_ref=dst, send_sem=send, recv_sem=recv,
            device_id={"tp": target}, device_id_type=pl.DeviceIdType.MESH,
        )

    def onward(block):
        low = block < half
        return remote(
            share.at[rows_for(across), columns(block)], passing.at[:, columns(block)],
            share_send.at[0, block], passing_sem.at[block], left if low else right,
        )

    def direct(block):
        low = block < half
        return remote(
            share.at[rows_for(right if low else left), columns(block)],
            (from_left if low else from_right).at[:, columns(block)],
            share_send.at[1, block], (left_sem if low else right_sem).at[block], right if low else left,
        )

    def summed(block):
        low = block < half
        return remote(
            passed.at[:, columns(block)], (from_right if low else from_left).at[:, columns(block)],
            passed_send.at[block], (right_sem if low else left_sem).at[block], left if low else right,
        )

    for block in BLOCK_ORDER:
        part = lax.dot_general(att_ref[...], att_rows[columns(block), :], NT, preferred_element_type=F32)
        part = part + lax.dot_general(conv_ref[...], conv_rows[columns(block), :], NT, preferred_element_type=F32)
        share[:, columns(block)] = part.astype(BF16)
        onward(block).start()
        direct(block).start()
    for block in BLOCK_ORDER:
        onward(block).wait_recv()
        mine = share[rows_for(left if block < half else right), columns(block)]
        passed[:, columns(block)] = (mine.astype(F32) + passing[:, columns(block)].astype(F32)).astype(BF16)
        summed(block).start()
    for block in BLOCK_ORDER:
        direct(block).wait_recv()
        summed(block).wait_recv()
        total = share[rows_for(tp), columns(block)].astype(F32) + from_left[:, columns(block)].astype(F32)
        out_ref[:, columns(block)] = (total + from_right[:, columns(block)].astype(F32)).astype(BF16)
    for block in range(OUT_BLOCKS):
        onward(block).wait_send()
        direct(block).wait_send()
        summed(block).wait_send()


def mixed_rows(attended, convolved, att_rows, conv_rows):
    count, features = attended.shape[0], att_rows.shape[0]
    rows = count // 4
    vmem = pl.BlockSpec(memory_space=pltpu.VMEM)
    slab = pltpu.VMEM((rows, features), BF16)
    sems = pltpu.SemaphoreType.DMA((OUT_BLOCKS,))
    return pl.pallas_call(
        output_kernel,
        name="output",
        out_shape=jax.ShapeDtypeStruct((rows, features), BF16),
        in_specs=[vmem] * 4,
        out_specs=vmem,
        scratch_shapes=[
            pltpu.VMEM((count, features), BF16), slab, slab, slab, slab,
            pltpu.SemaphoreType.DMA((2, OUT_BLOCKS)), sems, sems, sems, sems,
        ],
        compiler_params=pltpu.CompilerParams(
            collective_id=3, has_side_effects=True, vmem_limit_bytes=24 * 1024 * 1024
        ),
    )(attended, convolved, att_rows, conv_rows)


def local(
    tokens,
    norm_gain,
    w_query,
    w_key,
    w_value,
    score_shift,
    w_conv_b,
    w_conv_c,
    w_conv_u,
    conv_kernel,
    w_out_att,
    w_out_conv,
):
    rows, att_rows, conv_rows = gathered_rows(tokens, w_out_att, w_out_conv)
    normed = normalize(rows, norm_gain)
    keys, values = [
        jnp.dot(normed, weight, preferred_element_type=jnp.float32).astype(jnp.bfloat16)
        for weight in (w_key, w_value)
    ]
    key_whole, value_whole, queries, gate_b, gate_c, inputs_u = gathered_keys(
        keys, values, normed, (w_query, w_conv_b, w_conv_c, w_conv_u)
    )
    tok_count, conv_local = gate_b.shape
    products = (gate_c.astype(jnp.float32) * inputs_u.astype(jnp.float32)).astype(jnp.bfloat16)
    previous = shifted(products[tok_count - (CONV_K - 1) :], "sp", 1)
    attended, sums_all = attend(queries, key_whole, value_whole, score_shift)
    log_weight = jnp.log(jnp.maximum(-jnp.expm1(-sums_all), 0.05)).T
    extended = jnp.concatenate([previous, products], axis=0)
    summed = jnp.zeros((tok_count, conv_local), jnp.float32)
    for tap in range(CONV_K):
        summed = summed + conv_kernel[tap][None, :] * extended[tap : tap + tok_count].astype(
            jnp.float32
        )
    convolved = (gate_b.astype(jnp.float32) * summed).astype(jnp.bfloat16)
    mixed = mixed_rows(attended, convolved, att_rows, conv_rows)
    return (mixed, log_weight)


def solution(mesh):
    return jax.shard_map(
        local,
        mesh=mesh,
        in_specs=(
            P(("sp", "tp"), None),
            P(),
            P(None, "tp"),
            P(None, "tp"),
            P(None, "tp"),
            P("tp"),
            P(None, "tp"),
            P(None, "tp"),
            P(None, "tp"),
            P(None, "tp"),
            P("sp", "tp"),
            P("sp", "tp"),
        ),
        out_specs=(P(("sp", "tp"), None), P("sp", "tp")),
        check_vma=False,
    )
```

```python
import jax
import jax.numpy as jnp
from jax import lax
from jax.experimental import pallas as pl
from jax.experimental.pallas import tpu as pltpu
from jax.sharding import PartitionSpec as P

HEAD_DIM = 128
CONV_K = 3
F32 = jnp.float32
BF16 = jnp.bfloat16


def shifted(value, axis, steps):
    count = lax.axis_size(axis)
    leading, last = (max(0, -steps), min(count, count - steps))
    return lax.ppermute(value, axis, [(source, source + steps) for source in range(leading, last)])


def normalize(tokens, norm_gain):
    widened = tokens.astype(jnp.float32)
    inverse = lax.rsqrt(jnp.mean(widened * widened, axis=-1, keepdims=True) + 1e-06)
    return (widened * inverse * norm_gain).astype(jnp.bfloat16)


TILE = 256
NT = (((1,), (1,)), ((), ()))


def softplus(z):
    small = jnp.exp(-jnp.abs(z))
    whole = 1.0 + small
    return jnp.maximum(z, 0.0) + (jnp.log(whole) + (small - (whole - 1.0)))


def attention_kernel(
    q_ref, k_ref, v_ref, shift_ref, later_ref, out_ref, sum_ref, q_split, acc, carry, score, base, after
):
    last = lax.axis_index("sp")
    heads = [pl.ds(0, TILE), pl.ds(TILE, TILE)]
    for h in range(2):
        scaled = q_ref[:, h * HEAD_DIM : (h + 1) * HEAD_DIM].astype(F32) * HEAD_DIM ** (-0.5)
        high = scaled.astype(BF16)
        q_split[heads[h], 0:HEAD_DIM] = high
        q_split[heads[h], HEAD_DIM : 2 * HEAD_DIM] = (scaled - high.astype(F32)).astype(BF16)
    acc[...] = jnp.zeros_like(acc)
    carry[...] = jnp.zeros_like(carry)

    def rows_of(tile):
        return pl.ds(pl.multiple_of(jnp.maximum(tile, 0) * TILE, TILE), TILE)

    def scores(tile, slot):
        key = k_ref[rows_of(tile), :]
        twice = jnp.concatenate([key, key], axis=1)
        for h in range(2):
            score[slot, heads[h], :] = (
                lax.dot_general(q_split[heads[h], :], twice, NT, preferred_element_type=F32)
                + shift_ref[h]
            )

    def sums(slot, masked=False):
        for h in range(2):
            z = score[slot, heads[h], :]
            soft = softplus(z)
            if masked:
                row = lax.broadcasted_iota(jnp.int32, (TILE, TILE), 0)
                col = lax.broadcasted_iota(jnp.int32, (TILE, TILE), 1)
                soft = jnp.where(col < row, soft, 0.0)
                z = jnp.where(col < row, z, -jnp.inf)
            held = carry[heads[h], :]
            base[slot, heads[h], :] = (z - soft) - jnp.concatenate([held, held], axis=1)
            after[slot, heads[h], :] = jnp.dot(
                soft.astype(BF16), later_ref[...], preferred_element_type=F32
            )
            carry[heads[h], :] = held + jnp.sum(soft, axis=1, keepdims=True)

    def weigh(tile, slot):
        value = v_ref[rows_of(tile), :]
        for h in range(2):
            weight = jnp.exp(base[slot, heads[h], :] - after[slot, heads[h], :])
            acc[heads[h], :] += jnp.dot(weight.astype(BF16), value, preferred_element_type=F32)

    scores(last, 0)
    sums(0, True)
    scores(last - 1, 1)

    def two_tiles(step, _):
        tile = last - 1 - 2 * step
        scores(tile - 1, 0)
        sums(1)
        weigh(tile + 1, 0)
        scores(tile - 2, 1)
        sums(0)
        weigh(tile, 1)
        return 0

    lax.fori_loop(0, last // 2, two_tiles, 0)

    @pl.when(last % 2 == 1)
    def _():
        sums(1)
        weigh(1, 0)
        weigh(0, 1)

    @pl.when(last % 2 == 0)
    def _():
        weigh(0, 0)

    for h in range(2):
        out_ref[:, h * HEAD_DIM : (h + 1) * HEAD_DIM] = acc[heads[h], :].astype(BF16)
        sum_ref[h : h + 1, :] = jnp.transpose(carry[heads[h], :])[0:1, :]


def attend(queries, key_whole, value_whole, score_shift):
    row_count, width = queries.shape
    later = (jnp.arange(TILE)[:, None] > jnp.arange(TILE)[None, :]).astype(BF16)
    vmem = pl.BlockSpec(memory_space=pltpu.VMEM)
    attended, sums = pl.pallas_call(
        attention_kernel,
        name="attention",
        out_shape=(
            jax.ShapeDtypeStruct((row_count, width), BF16),
            jax.ShapeDtypeStruct((2, row_count), F32),
        ),
        in_specs=[vmem, vmem, vmem, pl.BlockSpec(memory_space=pltpu.SMEM), vmem],
        out_specs=(vmem, vmem),
        scratch_shapes=[
            pltpu.VMEM((2 * TILE, 2 * HEAD_DIM), BF16),
            pltpu.VMEM((2 * TILE, HEAD_DIM), F32),
            pltpu.VMEM((2 * TILE, HEAD_DIM), F32),
            pltpu.VMEM((2, 2 * TILE, TILE), F32),
            pltpu.VMEM((2, 2 * TILE, TILE), F32),
            pltpu.VMEM((2, 2 * TILE, TILE), F32),
        ],
        compiler_params=pltpu.CompilerParams(vmem_limit_bytes=16 * 1024 * 1024),
        cost_estimate=pl.CostEstimate(
            flops=12 * 10**9, bytes_accessed=9 * 10**6, transcendentals=25 * 10**6
        ),
    )(queries, key_whole, value_whole, score_shift, later)
    return attended, sums


UP, DOWN, NEXT, BACK, OTHER = range(5)
ZS, YS, CORES = 8, 4, 2


def plan():
    sends = {}
    for dz in range(-3, 5):
        for dy in range(-1, 3):
            first, second = [], []
            if dy == 0:
                if 0 <= dz < 4:
                    first.append((UP, dz + 1, 0))
                if -3 < dz <= 0:
                    first.append((DOWN, dz - 1, 0))
                first += [(NEXT, dz, 1), (BACK, dz, -1)]
            if dy == 1 and dz % 2 == 0:
                first.append((NEXT, dz, 2))
            if dy == -1 and dz % 2 == 1:
                first.append((BACK, dz, 2))
            if dz == 0:
                if dy == 0:
                    second += [(NEXT, 0, 1), (BACK, 0, -1)]
                if dy == 1:
                    second.append((NEXT, 0, 2))
            if 0 <= dz < 3 or (dz == 3 and dy % 2 == 0):
                second.append((UP, dz + 1, dy))
            if -3 < dz <= 0:
                second.append((DOWN, dz - 1, dy))
            if dz == -3 and dy % 2 == 1:
                second.append((DOWN, 4, dy))
            sends[0, dz, dy] = first
            sends[1, dz, dy] = second
    order = sorted(
        (key for key in sends if key[1:] != (0, 0)),
        key=lambda key: (abs(key[1]) + abs(key[2]), abs(key[2]) if key[0] == 0 else abs(key[1]), key),
    )
    return sends, order


def chunk_of(dz, dy):
    return (dz + 3) * YS + dy + 1


class Gather:
    def __init__(self, own, whole, rows, here_sem, side_sem, send_sem):
        self.own, self.whole, self.rows = own, whole, rows
        self.here_sem, self.side_sem, self.send_sem = here_sem, side_sem, send_sem
        sp = lax.axis_index("sp")
        self.z, self.y, self.core = sp // (YS * CORES), (sp // CORES) % YS, sp % CORES
        self.sends, self.order = plan()

    def sp_of(self, z, y, core):
        return (((z + ZS) % ZS) * YS + (y + YS) % YS) * CORES + core

    def neighbour(self, way):
        z, y, core = self.z, self.y, self.core
        return {
            UP: self.sp_of(z + 1, y, core),
            DOWN: self.sp_of(z - 1, y, core),
            NEXT: self.sp_of(z, y + 1, core),
            BACK: self.sp_of(z, y - 1, core),
            OTHER: self.sp_of(z, y, 1 - core),
        }[way]

    def slot(self, half, dz, dy, core):
        origin = self.sp_of(self.z - dz, self.y - dy, core)
        return self.whole[half].at[pl.ds(pl.multiple_of(origin * self.rows, self.rows), self.rows), :]

    def copy(self, half, dz, dy, way, sem):
        dst = self.slot(half, dz, dy, self.core)
        src = self.own[half] if (dz, dy) == (0, 0) else dst
        return pltpu.make_async_remote_copy(
            src_ref=src,
            dst_ref=dst,
            send_sem=self.send_sem.at[half],
            recv_sem=sem,
            device_id={"sp": self.neighbour(way)},
            device_id_type=pl.DeviceIdType.MESH,
        )

    def pass_on(self, half, dz, dy):
        for way, to_dz, to_dy in self.sends[half, dz, dy]:
            self.copy(half, dz, dy, way, self.here_sem.at[half, chunk_of(to_dz % 8 - 8 * (to_dz % 8 > 4), to_dy)]).start()
        self.copy(half, dz, dy, OTHER, self.side_sem.at[half, dz + 3]).start()

    def begin(self):
        for half, ways in ((0, (UP, DOWN)), (1, (NEXT, BACK)), (0, (NEXT, BACK)), (1, (UP, DOWN))):
            for way, to_dz, to_dy in self.sends[half, 0, 0]:
                if way in ways:
                    self.copy(half, 0, 0, way, self.here_sem.at[half, chunk_of(to_dz, to_dy)]).start()
        for half in range(2):
            self.copy(half, 0, 0, OTHER, self.side_sem.at[half, 3]).start()

    def arrive(self, key):
        half, dz, dy = key
        self.copy(half, dz, dy, UP, self.here_sem.at[half, chunk_of(dz, dy)]).wait_recv()
        self.pass_on(half, dz, dy)

    def side(self, half, dz):
        plane = self.whole[half].at[pl.ds(0, YS * self.rows), :]
        pltpu.make_async_copy(plane, plane, self.side_sem.at[half, dz + 3]).wait()

    def finish(self):
        for half in range(2):
            sent = self.whole[half].at[pl.ds(0, (ZS * YS * CORES - 1) * self.rows), :]
            pltpu.make_async_copy(sent, sent, self.send_sem.at[half]).wait()


def greet(gather, around=()):
    barrier = pltpu.get_barrier_semaphore()
    targets = [{"sp": gather.neighbour(way)} for way in (UP, DOWN, NEXT, BACK, OTHER)] + list(around)
    for target in targets:
        pl.semaphore_signal(barrier, inc=1, device_id=target, device_id_type=pl.DeviceIdType.MESH)
    pl.semaphore_wait(barrier, len(targets))


GATHER_SEMS = (
    pltpu.SemaphoreType.DMA((2, ZS * YS)),
    pltpu.SemaphoreType.DMA((2, ZS)),
    pltpu.SemaphoreType.DMA((2,)),
)


PROJECT_AFTER = (0, 0, 0, 0)


def keys_kernel(
    key_ref, value_ref, normed_ref, wq_ref, wb_ref, wc_ref, wu_ref,
    key_out, value_out, query_out, gate_b_out, gate_c_out, input_out,
    here_sem, side_sem, send_sem, own_sem,
):
    gather = Gather((key_ref, value_ref), (key_out, value_out), key_ref.shape[0], here_sem, side_sem, send_sem)
    weights = (wq_ref, wb_ref, wc_ref, wu_ref)
    greet(gather)
    gather.begin()
    kept = [
        pltpu.make_async_copy(gather.own[half], gather.slot(half, 0, 0, gather.core), own_sem.at[half])
        for half in range(2)
    ]
    for copy in kept:
        copy.start()
    outs = (query_out, gate_b_out, gate_c_out, input_out)
    for position, key in enumerate(gather.order):
        for number in [n for n in range(4) if PROJECT_AFTER[n] == position]:
            outs[number][...] = jnp.dot(
                normed_ref[...], weights[number][...], preferred_element_type=F32
            ).astype(BF16)
        gather.arrive(key)
    for half in range(2):
        for dz in range(-3, 5):
            gather.side(half, dz)
    for copy in kept:
        copy.wait()
    gather.finish()


def gathered_keys(keys, values, normed, weights):
    shape = (keys.shape[0] * ZS * YS * CORES, keys.shape[1])
    vmem = pl.BlockSpec(memory_space=pltpu.VMEM)
    projected = jax.ShapeDtypeStruct((normed.shape[0], weights[0].shape[1]), BF16)
    return pl.pallas_call(
        keys_kernel,
        name="gather_keys",
        out_shape=(jax.ShapeDtypeStruct(shape, BF16),) * 2 + (projected,) * 4,
        in_specs=[vmem] * 7,
        out_specs=(vmem,) * 6,
        scratch_shapes=[
            *GATHER_SEMS,
            pltpu.SemaphoreType.DMA((2,)),
        ],
        compiler_params=pltpu.CompilerParams(
            collective_id=1, has_side_effects=True, vmem_limit_bytes=24 * 1024 * 1024
        ),
    )(keys, values, normed, *weights)


def tokens_kernel(
    tokens_ref, att_ref, conv_ref, rows_out, att_out, conv_out,
    here_sem, side_sem, send_sem, own_sem, ring_sem, ring_send,
):
    gather = Gather((att_ref, conv_ref), (att_out, conv_out), att_ref.shape[0], here_sem, side_sem, send_sem)
    tp, count = lax.axis_index("tp"), 4
    right, left = {"tp": (tp + 1) % count}, {"tp": (tp + count - 1) % count}
    greet(gather, (right, left))
    rows = tokens_ref.shape[0]
    part = rows // 2

    def piece(origin, at):
        return rows_out.at[pl.ds(pl.multiple_of(((origin + count) % count) * rows + at * part, part), part), :]

    def ring(origin, at, target, number, mine):
        return pltpu.make_async_remote_copy(
            src_ref=tokens_ref.at[pl.ds(at * part, part), :] if mine else piece(origin, at),
            dst_ref=piece(origin, at),
            send_sem=ring_send.at[number],
            recv_sem=ring_sem.at[number],
            device_id=target,
            device_id_type=pl.DeviceIdType.MESH,
        )

    sent = [ring(tp, 0, right, 0, True), ring(tp, 1, left, 2, True), ring(tp, 1, right, 1, True), ring(tp, 0, left, 3, True)]
    for copy in sent:
        copy.start()
    gather.begin()
    kept = [
        pltpu.make_async_copy(gather.own[half], gather.slot(half, 0, 0, gather.core), own_sem.at[half])
        for half in range(2)
    ]
    kept.append(
        pltpu.make_async_copy(tokens_ref, rows_out.at[pl.ds(pl.multiple_of(tp * rows, rows), rows), :], own_sem.at[2])
    )
    for copy in kept:
        copy.start()
    for position, key in enumerate(gather.order):
        if position == 20:
            ring(tp - 1, 0, right, 0, False).wait_recv()
            sent.append(ring(tp - 1, 0, right, 4, False))
            sent[-1].start()
            ring(tp + 1, 1, left, 2, False).wait_recv()
            sent.append(ring(tp + 1, 1, left, 5, False))
            sent[-1].start()
        gather.arrive(key)
    for number, (origin, at) in enumerate(((tp - 1, 1), (tp + 1, 0), (tp - 2, 0), (tp + 2, 1))):
        ring(origin, at, right, (1, 3, 4, 5)[number], False).wait_recv()
    for half in range(2):
        for dz in range(-3, 5):
            gather.side(half, dz)
    for copy in kept:
        copy.wait()
    for copy in sent:
        copy.wait_send()
    gather.finish()


def gathered_rows(tokens, w_out_att, w_out_conv):
    vmem = pl.BlockSpec(memory_space=pltpu.VMEM)
    many = ZS * YS * CORES
    return pl.pallas_call(
        tokens_kernel,
        name="gather_rows",
        out_shape=(
            jax.ShapeDtypeStruct((tokens.shape[0] * 4, tokens.shape[1]), BF16),
            jax.ShapeDtypeStruct((w_out_att.shape[0] * many, w_out_att.shape[1]), BF16),
            jax.ShapeDtypeStruct((w_out_conv.shape[0] * many, w_out_conv.shape[1]), BF16),
        ),
        in_specs=[pl.BlockSpec(memory_space=pltpu.HBM)] * 3,
        out_specs=(vmem,) * 3,
        scratch_shapes=[
            *GATHER_SEMS,
            pltpu.SemaphoreType.DMA((3,)),
            pltpu.SemaphoreType.DMA((6,)),
            pltpu.SemaphoreType.DMA((6,)),
        ],
        compiler_params=pltpu.CompilerParams(
            collective_id=2, has_side_effects=True, vmem_limit_bytes=24 * 1024 * 1024
        ),
    )(tokens, w_out_att, w_out_conv)


OUT_BLOCKS = 8
BLOCK_ORDER = (0, 4, 1, 5, 2, 6, 3, 7)


def output_kernel(
    att_ref, conv_ref, att_rows, conv_rows, out_ref, share, from_left, from_right, passing, passed,
    share_send, passed_send, left_sem, right_sem, passing_sem,
):
    tp, count = lax.axis_index("tp"), 4
    right, left = (tp + 1) % count, (tp + count - 1) % count
    across = (tp + 2) % count
    barrier = pltpu.get_barrier_semaphore()
    for target in (left, right):
        pl.semaphore_signal(barrier, inc=1, device_id={"tp": target}, device_id_type=pl.DeviceIdType.MESH)
    pl.semaphore_wait(barrier, 2)
    rows = out_ref.shape[0]
    width = out_ref.shape[1] // OUT_BLOCKS
    half = OUT_BLOCKS // 2

    def columns(block):
        return pl.ds(block * width, width)

    def rows_for(target):
        return pl.ds(pl.multiple_of(target * rows, rows), rows)

    def remote(src, dst, send, recv, target):
        return pltpu.make_async_remote_copy(
            src_ref=src, dst_ref=dst, send_sem=send, recv_sem=recv,
            device_id={"tp": target}, device_id_type=pl.DeviceIdType.MESH,
        )

    def onward(block):
        low = block < half
        return remote(
            share.at[rows_for(across), columns(block)], passing.at[:, columns(block)],
            share_send.at[0, block], passing_sem.at[block], left if low else right,
        )

    def direct(block):
        low = block < half
        return remote(
            share.at[rows_for(right if low else left), columns(block)],
            (from_left if low else from_right).at[:, columns(block)],
            share_send.at[1, block], (left_sem if low else right_sem).at[block], right if low else left,
        )

    def summed(block):
        low = block < half
        return remote(
            passed.at[:, columns(block)], (from_right if low else from_left).at[:, columns(block)],
            passed_send.at[block], (right_sem if low else left_sem).at[block], left if low else right,
        )

    for block in BLOCK_ORDER:
        part = lax.dot_general(att_ref[...], att_rows[columns(block), :], NT, preferred_element_type=F32)
        part = part + lax.dot_general(conv_ref[...], conv_rows[columns(block), :], NT, preferred_element_type=F32)
        share[:, columns(block)] = part.astype(BF16)
        onward(block).start()
        direct(block).start()
    for block in BLOCK_ORDER:
        onward(block).wait_recv()
        mine = share[rows_for(left if block < half else right), columns(block)]
        passed[:, columns(block)] = (mine.astype(F32) + passing[:, columns(block)].astype(F32)).astype(BF16)
        summed(block).start()
    for block in BLOCK_ORDER:
        direct(block).wait_recv()
        summed(block).wait_recv()
        total = share[rows_for(tp), columns(block)].astype(F32) + from_left[:, columns(block)].astype(F32)
        out_ref[:, columns(block)] = (total + from_right[:, columns(block)].astype(F32)).astype(BF16)
    for block in range(OUT_BLOCKS):
        onward(block).wait_send()
        direct(block).wait_send()
        summed(block).wait_send()


def mixed_rows(attended, convolved, att_rows, conv_rows):
    count, features = attended.shape[0], att_rows.shape[0]
    rows = count // 4
    vmem = pl.BlockSpec(memory_space=pltpu.VMEM)
    slab = pltpu.VMEM((rows, features), BF16)
    sems = pltpu.SemaphoreType.DMA((OUT_BLOCKS,))
    return pl.pallas_call(
        output_kernel,
        name="output",
        out_shape=jax.ShapeDtypeStruct((rows, features), BF16),
        in_specs=[vmem] * 4,
        out_specs=vmem,
        scratch_shapes=[
            pltpu.VMEM((count, features), BF16), slab, slab, slab, slab,
            pltpu.SemaphoreType.DMA((2, OUT_BLOCKS)), sems, sems, sems, sems,
        ],
        compiler_params=pltpu.CompilerParams(
            collective_id=3, has_side_effects=True, vmem_limit_bytes=24 * 1024 * 1024
        ),
    )(attended, convolved, att_rows, conv_rows)


def local(
    tokens,
    norm_gain,
    w_query,
    w_key,
    w_value,
    score_shift,
    w_conv_b,
    w_conv_c,
    w_conv_u,
    conv_kernel,
    w_out_att,
    w_out_conv,
):
    rows, att_rows, conv_rows = gathered_rows(tokens, w_out_att, w_out_conv)
    normed = normalize(rows, norm_gain)
    keys, values = [
        jnp.dot(normed, weight, preferred_element_type=jnp.float32).astype(jnp.bfloat16)
        for weight in (w_key, w_value)
    ]
    key_whole, value_whole, queries, gate_b, gate_c, inputs_u = gathered_keys(
        keys, values, normed, (w_query, w_conv_b, w_conv_c, w_conv_u)
    )
    tok_count, conv_local = gate_b.shape
    products = (gate_c.astype(jnp.float32) * inputs_u.astype(jnp.float32)).astype(jnp.bfloat16)
    previous = shifted(products[tok_count - (CONV_K - 1) :], "sp", 1)
    attended, sums_all = attend(queries, key_whole, value_whole, score_shift)
    log_weight = jnp.log(jnp.maximum(-jnp.expm1(-sums_all), 0.05)).T
    extended = jnp.concatenate([previous, products], axis=0)
    summed = jnp.zeros((tok_count, conv_local), jnp.float32)
    for tap in range(CONV_K):
        summed = summed + conv_kernel[tap][None, :] * extended[tap : tap + tok_count].astype(
            jnp.float32
        )
    convolved = (gate_b.astype(jnp.float32) * summed).astype(jnp.bfloat16)
    mixed = mixed_rows(attended, convolved, att_rows, conv_rows)
    return (mixed, log_weight)


def solution(mesh):
    return jax.shard_map(
        local,
        mesh=mesh,
        in_specs=(
            P(("sp", "tp"), None),
            P(),
            P(None, "tp"),
            P(None, "tp"),
            P(None, "tp"),
            P("tp"),
            P(None, "tp"),
            P(None, "tp"),
            P(None, "tp"),
            P(None, "tp"),
            P("sp", "tp"),
            P("sp", "tp"),
        ),
        out_specs=(P(("sp", "tp"), None), P("sp", "tp")),
        check_vma=False,
    )
```
